32 devices in a mesh: sp: 8 (over z, core), tp: 4 (over y, x).
Axes of the slice: x: 2, y: 2, z: 4, core: 2. Of those that a mesh axis runs over, the one named last changes fastest.
Arguments:
- residual: bfloat16 [2048, 2048], P('sp'), may hold values from -6 to 6
- queries: bfloat16 [2048, 16, 128], P('sp', 'tp'), may hold values from -256 to 256
- key_vectors: bfloat16 [2048, 16, 128], P('sp', 'tp'), may hold values from -5.3 to 5.3
- value_rows: bfloat16 [2048, 16, 128], P('sp', 'tp'), may hold values from -6 to 6
- head_lambda: float32 [16], P('tp'), may hold values from 0.3 to 0.8
- head_gain: float32 [128], replicated, may hold values from 0.1 to 1.9
- out_weight: bfloat16 [2048, 2048], P('tp'), may hold values from -0.125 to 0.125
- ffn_gain: float32 [2048], replicated, may hold values from 0.1 to 1.9
- expert_gate: bfloat16 [8, 2048, 4096], P('sp', None, 'tp'), may hold values from -0.125 to 0.125
- expert_up: bfloat16 [8, 2048, 4096], P('sp', None, 'tp'), may hold values from -0.125 to 0.125
- expert_down: bfloat16 [8, 4096, 2048], P('sp', None, 'tp'), may hold values from -0.09375 to 0.09375
- routing: int32 [2048, 2], P('sp'), may hold values from 0 to 7, as said below
- route_weight: float32 [2048, 2], P('sp'), may hold values from 0.1 to 0.9
Outputs:
- layer_out: bfloat16 [2048, 2048], P('sp')
The draws below stay inside these ranges and needn't reach their ends.
Inputs may be any that keep to these rules, and one draw needn't show every extreme that they name: `routing`: each row names two different experts of one group of 2 consecutive experts. In each aligned block of 256 rows no expert is named by more than 128 rows, and in every block some expert is named by exactly 128 rows.
All inputs are finite; a program needn't handle non-finite values.
Results may differ from the reference program's by a relative error of at most 0.015.
Values may be sent and summed in bfloat16 or wider, within the bound.
A program may use at most 64 MiB of HBM per device.

```python
import math
import jax
import jax.numpy as jnp
from jax import lax

D = 2048
HEADS = 16
QK = 64
HV = 128
FF = 4096
GROUPS = 4
TOP = 2
T_SP = 256
SEQ = 2048
EXPERTS = 8
CAP = 128
N_SP = 8


def drawn(key):
    spread = 1.3
    base_key, query_key = jax.random.split(jax.random.fold_in(key, 5), 2)
    width = 2 * QK
    key_array = spread * jax.random.truncated_normal(base_key, -4.0, 4.0, (SEQ, HEADS, width), jnp.float32)
    query_array = spread * jax.random.truncated_normal(query_key, -4.0, 4.0, (SEQ, HEADS, width), jnp.float32)
    return (query_array, key_array)


def draw_queries(key, part):
    return drawn(key)[0].astype(jnp.bfloat16)


def draw_key_vectors(key, part):
    return drawn(key)[1].astype(jnp.bfloat16)


def draw_routing(key, part):
    per_group = EXPERTS // GROUPS
    block_count = SEQ // T_SP
    order_key, inner_key, rank_key = jax.random.split(jax.random.fold_in(key, 11), 3)
    group_order = jax.random.permutation(order_key, GROUPS).astype(jnp.int32)
    inner_order = jax.vmap(lambda sub_key: jax.random.permutation(sub_key, per_group))(jax.random.split(inner_key, GROUPS)).astype(jnp.int32)
    rank_table = jax.vmap(lambda sub_key: jax.random.permutation(sub_key, T_SP))(jax.random.split(rank_key, block_count)).astype(jnp.int32).reshape(-1)
    half_mark = T_SP // 2
    rank_level = (rank_table >= half_mark).astype(jnp.int32) + (rank_table >= half_mark + T_SP // 4).astype(jnp.int32) + (rank_table >= half_mark + T_SP // 4 + T_SP // 8).astype(jnp.int32)
    offsets = jnp.array([0, T_SP // 2, 3 * T_SP // 4, 7 * T_SP // 8], jnp.int32)
    within = rank_table - offsets[rank_level]
    first_pick = within % per_group
    step_size = 1 + within // per_group % max(per_group - 1, 1)
    second_pick = (first_pick + step_size) % per_group
    group_id = group_order[rank_level]
    first_expert = group_id * per_group + inner_order[group_id, first_pick]
    second_expert = group_id * per_group + inner_order[group_id, second_pick]
    return jnp.stack([first_expert, second_expert], axis=1).astype(jnp.int32)


def block_levels(rng, shape, shards, least, high):
    loudness = 1.0
    for axis_at, parts in shards:
        draws = jax.random.uniform(jax.random.fold_in(jax.random.fold_in(rng, 6), axis_at), (parts,), jnp.float32, least / len(shards), high / len(shards))
        loudness = loudness * jnp.repeat(jnp.exp(draws), shape[axis_at] // parts).reshape((-1,) + (1,) * (len(shape) - 1 - axis_at))
    return loudness


def scatter_about(rng, extent, scale, most, cuts=(), held_as=jnp.bfloat16):
    level = block_levels(rng, extent, cuts, -0.22, 0.18) if cuts else 1.0
    drawn = jax.random.normal(rng, extent, jnp.float32) * scale * level
    return jnp.minimum(jnp.maximum(drawn, -most), most).astype(held_as)


def setup_inputs(seed: int = 0) -> dict:
    keys = jax.random.split(jax.random.key(seed), 14)
    residual = scatter_about(keys[0], (SEQ, D), 1.0, 6.0, ((0, 8),))
    queries = draw_queries(jax.random.fold_in(keys[13], 71), 0)
    key_vectors = draw_key_vectors(jax.random.fold_in(keys[13], 71), 0)
    value_rows = scatter_about(keys[3], (SEQ, HEADS, HV), 1.0, 6.0, ((0, 8), (1, 4)))
    head_lambda = jnp.clip(0.3 + 0.5 * jax.random.uniform(keys[4], (HEADS,), jnp.float32) ** block_levels(keys[4], (HEADS,), ((0, 4),), -0.2, 0.2), 0.3, 0.8)
    head_gain = jnp.clip(1.0 + 0.18 * jax.random.normal(keys[5], (HV,), jnp.float32), 0.1, 1.9)
    out_weight = scatter_about(keys[6], (HEADS * HV, D), (HEADS * HV) ** -0.5, 0.125, ((0, 4),))
    ffn_gain = jnp.clip(1.0 + 0.18 * jax.random.normal(keys[7], (D,), jnp.float32), 0.1, 1.9)
    expert_gate = scatter_about(keys[8], (EXPERTS, D, FF), D ** -0.5, 0.125, ((0, 8), (2, 4)))
    expert_up = scatter_about(keys[9], (EXPERTS, D, FF), D ** -0.5, 0.125, ((0, 8), (2, 4)))
    expert_down = scatter_about(keys[10], (EXPERTS, FF, D), FF ** -0.5, 0.09375, ((0, 8), (2, 4)))
    routing = draw_routing(jax.random.fold_in(keys[13], 71), 0)
    route_weight = jnp.clip(0.1 + 0.79999997 * jax.random.uniform(keys[12], (SEQ, TOP), jnp.float32) ** block_levels(keys[12], (SEQ, TOP), ((0, 8),), -0.2, 0.2), 0.1, 0.9)
    return {"residual": residual, "queries": queries, "key_vectors": key_vectors, "value_rows": value_rows, "head_lambda": head_lambda, "head_gain": head_gain, "out_weight": out_weight, "ffn_gain": ffn_gain, "expert_gate": expert_gate, "expert_up": expert_up, "expert_down": expert_down, "routing": routing, "route_weight": route_weight}


norm_eps = 1e-06

def differential(queries, key_vectors, value_rows, head_lambda, head_gain):
    seq_len = queries.shape[0]
    block_len = math.gcd(seq_len, 512)
    score_scale = QK ** (-0.5)
    key_float = key_vectors.astype(jnp.float32)
    value_float = value_rows.astype(jnp.float32)
    key_pos = jnp.arange(seq_len, dtype=jnp.int32)

    def one_map(query_part, key_part, query_pos):
        scores = jnp.einsum('qhd,khd->hqk', query_part, key_part) * score_scale
        masked = jnp.where(key_pos[None, None, :] <= query_pos[None, :, None], scores, -jnp.inf)
        highest = lax.optimization_barrier(jnp.max(masked, axis=-1, keepdims=True))
        weights = jnp.exp(masked - highest)
        totals = lax.optimization_barrier(jnp.sum(weights, axis=-1))
        rounded = lax.optimization_barrier(weights.astype(jnp.bfloat16)).astype(jnp.float32)
        blended = jnp.einsum('hqk,khe->qhe', rounded, value_float)
        return blended / jnp.transpose(totals)[:, :, None]

    def one_block(block_index):
        first_row = block_index * block_len
        query_rows = lax.dynamic_slice_in_dim(queries, first_row, block_len, 0).astype(jnp.float32)
        query_pos = first_row + jnp.arange(block_len, dtype=jnp.int32)
        first_map = one_map(query_rows[:, :, :QK], key_float[:, :, :QK], query_pos)
        second_map = one_map(query_rows[:, :, QK:], key_float[:, :, QK:], query_pos)
        return first_map - head_lambda[None, :, None] * second_map
    blocks_out = lax.map(one_block, jnp.arange(seq_len // block_len, dtype=jnp.int32))
    combined = blocks_out.reshape(seq_len, HEADS, HV)
    normed = combined * lax.rsqrt(lax.optimization_barrier(jnp.mean(combined * combined, axis=-1, keepdims=True)) + norm_eps) * head_gain
    return normed.astype(jnp.bfloat16).reshape(seq_len, HEADS * HV)

def reference(residual, queries, key_vectors, value_rows, head_lambda, head_gain, out_weight, ffn_gain, expert_gate, expert_up, expert_down, routing, route_weight):
    attended = differential(queries, key_vectors, value_rows, head_lambda, head_gain)
    stream = residual.astype(jnp.float32) + jnp.dot(attended, out_weight, preferred_element_type=jnp.float32)
    normed = (stream * lax.rsqrt(lax.optimization_barrier(jnp.mean(stream * stream, axis=-1, keepdims=True)) + norm_eps) * ffn_gain).astype(jnp.bfloat16)
    slot_count = N_SP * CAP

    def expert_step(totals, stacked):
        gate_weight, up_weight, down_weight, expert_id = stacked
        chosen = jnp.any(routing == expert_id, axis=1)
        token_ids = jnp.nonzero(chosen, size=slot_count, fill_value=0)[0].astype(jnp.int32)
        live_slot = jnp.arange(slot_count, dtype=jnp.int32) < jnp.sum(chosen.astype(jnp.int32))
        picked = normed[token_ids]
        gate_part = jnp.dot(picked, gate_weight, preferred_element_type=jnp.float32)
        up_part = jnp.dot(picked, up_weight, preferred_element_type=jnp.float32)
        inner_act = (jax.nn.silu(gate_part) * up_part).astype(jnp.bfloat16)
        result = jnp.dot(inner_act, down_weight, preferred_element_type=jnp.float32).astype(jnp.bfloat16)
        factor = lax.optimization_barrier(jnp.sum(jnp.where(routing[token_ids] == expert_id, route_weight[token_ids], jnp.zeros_like(route_weight[token_ids])), axis=1))
        factor = jnp.where(live_slot, factor, jnp.zeros_like(factor))
        return (totals.at[token_ids].add(factor[:, None] * result.astype(jnp.float32)), None)
    moe_sum, _ = lax.scan(expert_step, jnp.zeros((SEQ, D), jnp.float32), (expert_gate, expert_up, expert_down, jnp.arange(EXPERTS, dtype=jnp.int32)))
    return (stream + moe_sum).astype(jnp.bfloat16)
```

```python
import functools
import math

import jax
import jax.numpy as jnp
from jax import lax
from jax.experimental import pallas as pl
from jax.experimental.pallas import tpu as pltpu
from jax.sharding import PartitionSpec as P

GROUPS = 4
SC = jax.named_scope


norm_eps = 1e-06


def online_update(running, query_part, key_part, value_part, query_pos, key_pos, score_scale):
    highest, totals, accum = running
    scores = (
        jnp.einsum("qhd,khd->hqk", query_part, key_part, preferred_element_type=jnp.float32)
        * score_scale
    )
    scores = jnp.where(key_pos[None, None, :] <= query_pos[None, :, None], scores, -jnp.inf)
    new_high = jnp.maximum(highest, jnp.max(scores, axis=-1))
    shrink = jnp.exp(highest - new_high)
    weights = jnp.exp(scores - new_high[:, :, None])
    totals = shrink * totals + jnp.sum(weights, axis=-1)
    blended = jnp.einsum(
        "hqk,khe->qhe", weights.astype(jnp.bfloat16), value_part, preferred_element_type=jnp.float32
    )
    accum = jnp.transpose(shrink)[:, :, None] * accum + blended
    return (new_high, totals, accum)


def shards(
    residual,
    queries,
    key_vectors,
    value_rows,
    head_lambda,
    head_gain,
    out_weight,
    ffn_gain,
    expert_gate,
    expert_up,
    expert_down,
    routing,
    route_weight,
):
    tok_count = queries.shape[0]
    local_heads = queries.shape[1]
    half_width = queries.shape[2] // 2
    value_width = value_rows.shape[2]
    score_scale = half_width ** (-0.5)
    query_pos = lax.axis_index("sp") * tok_count + jnp.arange(tok_count, dtype=jnp.int32)
    last_query = query_pos[-1]
    first_half = queries[:, :, :half_width]
    second_half = queries[:, :, half_width:]
    start_high = jnp.full((local_heads, tok_count), -1e30, jnp.float32)
    start_total = jnp.zeros((local_heads, tok_count), jnp.float32)
    start_accum = jnp.zeros((tok_count, local_heads, value_width), jnp.float32)
    empty_state = (start_high, start_total, start_accum)
    running = (empty_state, empty_state)
    key_piece = lax.all_gather(key_vectors, "sp", axis=0, tiled=True)
    value_piece = lax.all_gather(value_rows, "sp", axis=0, tiled=True)
    piece_len = key_piece.shape[0]
    block_len = math.gcd(piece_len, 512)
    block_count = piece_len // block_len
    key_blocks = key_piece.reshape(block_count, block_len, local_heads, 2 * half_width)
    value_blocks = value_piece.reshape(block_count, block_len, local_heads, value_width)

    def visit(current, stacked):
        block_index, key_block, value_block = stacked
        block_first = block_index * block_len
        key_pos = block_first + jnp.arange(block_len, dtype=jnp.int32)

        def compute(inside):
            first_state = online_update(
                inside[0],
                first_half,
                key_block[:, :, :half_width],
                value_block,
                query_pos,
                key_pos,
                score_scale,
            )
            second_state = online_update(
                inside[1],
                second_half,
                key_block[:, :, half_width:],
                value_block,
                query_pos,
                key_pos,
                score_scale,
            )
            return (first_state, second_state)

        return (lax.cond(block_first <= last_query, compute, lambda inside: inside, current), None)

    running, _ = lax.scan(
        visit, running, (jnp.arange(block_count, dtype=jnp.int32), key_blocks, value_blocks)
    )
    first_state, second_state = running
    first_out = first_state[2] / jnp.transpose(first_state[1])[:, :, None]
    second_out = second_state[2] / jnp.transpose(second_state[1])[:, :, None]
    combined = first_out - head_lambda[None, :, None] * second_out
    normed_heads = (
        combined
        * lax.rsqrt(jnp.mean(combined * combined, axis=-1, keepdims=True) + norm_eps)
        * head_gain
    )
    attended = normed_heads.astype(jnp.bfloat16).reshape(tok_count, local_heads * value_width)
    partial_proj = jnp.dot(attended, out_weight, preferred_element_type=jnp.float32)
    projected = lax.psum(partial_proj.astype(jnp.bfloat16), "tp").astype(jnp.float32)
    stream = residual.astype(jnp.float32) + projected
    block_normed = (
        stream * lax.rsqrt(jnp.mean(stream * stream, axis=-1, keepdims=True) + norm_eps) * ffn_gain
    ).astype(jnp.bfloat16)
    expert_count = lax.axis_size("sp")
    tp_count = lax.axis_size("tp")
    per_group = expert_count // GROUPS
    capacity = tok_count // per_group
    top_count = routing.shape[1]
    model_width = block_normed.shape[1]
    flat_routes = routing.reshape(-1)
    route_count = flat_routes.shape[0]
    onehot = (flat_routes[:, None] == jnp.arange(expert_count, dtype=jnp.int32)[None, :]).astype(
        jnp.int32
    )
    earlier = jnp.cumsum(onehot, axis=0) - onehot
    position = jnp.sum(earlier * onehot, axis=1)
    slot_index = flat_routes * capacity + position
    slot_token = (
        jnp.full((expert_count * capacity,), tok_count, jnp.int32)
        .at[slot_index]
        .set(jnp.arange(route_count, dtype=jnp.int32) // top_count)
    )
    slot_table = slot_token.reshape(expert_count, capacity)
    slice_width = model_width // tp_count
    own_columns = lax.dynamic_slice_in_dim(
        block_normed, lax.axis_index("tp") * slice_width, slice_width, 1
    )
    outgoing = jnp.take(own_columns, slot_table, axis=0, mode="fill", fill_value=0)
    landed = lax.all_to_all(outgoing, "sp", split_axis=0, concat_axis=0, tiled=True)
    arrived = lax.all_gather(landed, "tp", axis=2, tiled=True)
    expert_rows = arrived.reshape(-1, model_width)
    gate_part = jnp.dot(expert_rows, expert_gate[0], preferred_element_type=jnp.float32)
    up_part = jnp.dot(expert_rows, expert_up[0], preferred_element_type=jnp.float32)
    inner_act = (jax.nn.silu(gate_part) * up_part).astype(jnp.bfloat16)
    down_width = expert_down.shape[2]
    weight_rows = expert_down[0]
    expert_sum = jnp.dot(
        lax.all_gather(inner_act, "tp", axis=1, tiled=True),
        weight_rows,
        preferred_element_type=jnp.float32,
    )
    expert_out = expert_sum.astype(jnp.bfloat16).reshape(expert_count, capacity, down_width)
    returned = lax.all_to_all(expert_out, "sp", split_axis=0, concat_axis=0, tiled=True)
    per_route = returned.reshape(expert_count * capacity, down_width)[slot_index]
    weighted = per_route.astype(jnp.float32) * route_weight.reshape(-1)[:, None]
    token_sum = jnp.sum(weighted.reshape(tok_count, top_count, down_width), axis=1)
    moe_rows = lax.all_gather(token_sum.astype(jnp.bfloat16), "tp", axis=1, tiled=True).astype(
        token_sum.dtype
    )
    return (stream + moe_rows).astype(jnp.bfloat16)


MESH = pl.DeviceIdType.MESH
F32 = jnp.float32
BF16 = jnp.bfloat16


def remote(src, dst, send_sem, recv_sem, sp, tp):
    return pltpu.make_async_remote_copy(
        src_ref=src,
        dst_ref=dst,
        send_sem=send_sem,
        recv_sem=recv_sem,
        device_id={"sp": sp, "tp": tp},
        device_id_type=MESH,
    )


def mixed_dot(left, right, contract):
    return lax.dot_general(left, right, (contract, ((), ())), preferred_element_type=F32)


def dispersed(value):
    high = value.astype(BF16)
    rest = value - high.astype(F32)
    middle = rest.astype(BF16)
    low = (rest - middle.astype(F32)).astype(BF16)
    return jnp.concatenate([high, middle, low], axis=0)


def exact_pick(value, picker):
    count = value.shape[0]
    parts = mixed_dot(dispersed(value), picker, ((1,), (0,)))
    return parts[:count] + parts[count : 2 * count] + parts[2 * count :]


def layer_kernel(
    n, tps, cap, heads, head_width,
    q_ref, k_ref, v_ref, route_ref, rw_ref, wd_ref, lam_ref, gain_ref, ow_ref, res_ref, fg_ref,
    gate_ref, up_ref,
    outv,
    raw, resv, owv, sel, selt, stream_ref, normed_ref, meta,
    xs, xall, wg, wu, wdv, hid, keep, away, near, rsend, rrecv, rpass, back, ret,
    kall, vall, rowm, qs, highs, totals, acc, att, part, rbuf, ppass, sq_send, sq_recv,
    in_sem, w_sem, x_send, x_tp, x_sib, x_recv, s_recv, n_send, n_recv, r_send, r_recv,
    b_send, b_recv, o_send, o_recv,
    kv_next, kv_sib, kv_recv, wd_send, wd_recv, m_send, m_recv,
    rs_send, rs_recv, sq_ss, sq_rs, free_sem,
):
    sp = lax.axis_index("sp")
    tp = lax.axis_index("tp")
    z, c = sp // 2, sp % 2
    zs = n // 2
    sib = 2 * z + 1 - c
    toks = resv.shape[0]
    width = heads * head_width
    half = head_width // 2
    piece = normed_ref.shape[1]
    wd_rows = wdv.shape[1]
    experts = n
    per_group = experts // GROUPS
    beside, above, across = tp ^ 1, tp ^ 2, tp ^ 3

    barrier = pltpu.get_barrier_semaphore()
    for d in range(1, n):
        pl.semaphore_signal(
            barrier, inc=1, device_id={"sp": (sp + d) % n, "tp": tp}, device_id_type=MESH
        )
    for d in range(1, tps):
        pl.semaphore_signal(
            barrier, inc=1, device_id={"sp": sp, "tp": (tp + d) % tps}, device_id_type=MESH
        )
    inputs = [
        pltpu.make_async_copy(k_ref, raw.at[0], in_sem.at[0]),
        pltpu.make_async_copy(v_ref, raw.at[1], in_sem.at[1]),
        pltpu.make_async_copy(q_ref, raw.at[2], in_sem.at[2]),
        pltpu.make_async_copy(ow_ref, owv, in_sem.at[3]),
        pltpu.make_async_copy(res_ref, resv, in_sem.at[4]),
    ]
    loads = [
        pltpu.make_async_copy(gate_ref.at[0], wg, w_sem.at[0]),
        pltpu.make_async_copy(up_ref.at[0], wu, w_sem.at[1]),
        pltpu.make_async_copy(
            wd_ref.at[pl.ds(pl.multiple_of(tp * wd_rows, wd_rows), wd_rows), :],
            wdv.at[tp], w_sem.at[2],
        ),
    ]
    for load in inputs + loads:
        load.start()

    run = toks // heads
    spot_row = lax.broadcasted_iota(jnp.int32, (run, toks), 0)
    spot_col = lax.broadcasted_iota(jnp.int32, (run, toks), 1)
    order = jnp.concatenate(
        [(spot_col == spot_row * heads + h).astype(BF16) for h in range(heads)], axis=0
    )

    def split(which, store):
        for i in range(heads):
            rows = jnp.dot(
                order, raw[which, i * toks : (i + 1) * toks, :], preferred_element_type=F32
            )
            for h in range(heads):
                store(i, h, rows[h * run : (h + 1) * run, :])

    def head_rows(h, i=0, count=toks):
        return slice(h * toks + i * run, h * toks + i * run + count)

    def store_keys(i, h, rows):
        kall[sp, head_rows(h, i, run), :] = rows.astype(BF16)

    def store_rows(i, h, rows):
        rowm[head_rows(h, i, run), :] = rows.astype(BF16)

    unit = (
        lax.broadcasted_iota(jnp.int32, (head_width, head_width), 0)
        == lax.broadcasted_iota(jnp.int32, (head_width, head_width), 1)
    ).astype(BF16)

    def turned(h):
        return mixed_dot(unit, rowm[head_rows(h), :], ((1,), (1,)))

    inputs[0].wait()
    split(0, store_keys)
    inputs[1].wait()
    split(1, store_rows)
    for h in range(heads):
        vall[sp, h * head_width : (h + 1) * head_width, :] = turned(h).astype(BF16)

    chunks = 8
    wd_run = wd_rows // chunks

    def wd_copy(k, d):
        to = tp ^ d
        return remote(
            wd_ref.at[pl.ds(pl.multiple_of(to * wd_rows + k * wd_run, wd_run), wd_run), :],
            wdv.at[tp, pl.ds(pl.multiple_of(k * wd_run, wd_run), wd_run)],
            wd_send, wd_recv, sp, to,
        )

    def by_plane(values):
        chosen = values[-1]
        for plane, value in enumerate(values[:-1]):
            chosen = jnp.where(z == plane, value, chosen)
        return chosen

    wd_points = [
        (0, 0, 0, 0), (1, 3, 5, 7), (2, 4, 6, 7), (3, 4, 6, 7), (6, 6, 8, 8), (7, 7, 8, 8), (8, 8, 8, 8)
    ]

    def wd_start(point):
        def start(k, carry):
            for d in (3, 1, 2):
                wd_copy(k, d).start()
            return carry

        lax.fori_loop(by_plane(wd_points[point - 1]), by_plane(wd_points[point]), start, 0)

    class KeyCopies:
        def __init__(self, b, sends, to):
            self.at = (sends.at[b], kv_recv.at[b], to, tp)
            self.block = b

        def start(self):
            for blocks in (kall, vall):
                here = blocks.at[self.block]
                remote(here, here, *self.at).start()

        def wait_send(self):
            both = kall.at[pl.ds(0, 2)]
            remote(both, both, *self.at).wait_send()

        def wait_recv(self):
            both = kall.at[pl.ds(0, 2)]
            remote(both, both, *self.at).wait_recv()

    def next_copy(b):
        return KeyCopies(b, kv_next, sp + 2)

    def kv_sib_copy(b):
        return KeyCopies(b, kv_sib, sib)

    with SC('barrier_wait'):
        pl.semaphore_wait(barrier, n - 1 + tps - 1)

    @pl.when(z < zs - 1)
    def _():
        next_copy(sp).start()

    @pl.when(c == 0)
    def _():
        kv_sib_copy(sp).start()

    wd_start(1)

    depth = lax.broadcasted_iota(jnp.int32, (head_width, toks), 0)
    scale = half ** (-0.5)
    inputs[2].wait()
    split(2, store_rows)
    for h in range(heads):
        columns = turned(h) * scale
        qs[h, :, 0:toks] = jnp.where(depth < half, columns, 0.0).astype(BF16)
        qs[h, :, toks:] = jnp.where(depth >= half, columns, 0.0).astype(BF16)
    highs[...] = jnp.full_like(highs, -1e30)
    totals[...] = jnp.zeros_like(totals)
    acc[...] = jnp.zeros_like(acc)
    rows = lax.broadcasted_iota(jnp.int32, (toks, toks), 0)
    cols = lax.broadcasted_iota(jnp.int32, (toks, toks), 1)
    eye = rows == cols

    def process(b, masked):
        for h in range(heads):
            scores = mixed_dot(kall[b, head_rows(h), :], qs[h], ((1,), (0,)))
            if masked:
                scores = jnp.where(jnp.concatenate([rows <= cols] * 2, axis=1), scores, -1e30)
            old = highs[h]
            high = jnp.maximum(old, jnp.max(scores, axis=0, keepdims=True))
            shrink = jnp.exp(old - high)
            weights = jnp.exp(scores - high)
            totals[h] = shrink * totals[h] + jnp.sum(weights, axis=0, keepdims=True)
            blended = mixed_dot(
                vall[b, h * head_width : (h + 1) * head_width, :], weights.astype(BF16),
                ((1,), (0,)),
            )
            acc[h] = shrink * acc[h] + blended
            highs[h] = high

    with SC('proc_own'):
        process(sp, True)

    first = route_ref[0:1, :]
    lead = lax.broadcasted_iota(jnp.int32, (8, toks), 0)
    member = jnp.logical_and(
        first >= lead * per_group, first < (lead + 1) * per_group
    ).astype(F32)
    earlier = mixed_dot(member.astype(BF16), (rows < cols).astype(BF16), ((1,), (0,)))
    slot = jnp.sum(member * (earlier + lead.astype(F32) * cap), axis=0, keepdims=True)
    slot_col = jnp.sum(jnp.where(eye, slot, 0.0), axis=1, keepdims=True)
    slots = GROUPS * cap
    sel[...] = (
        lax.broadcasted_iota(jnp.int32, (slots, toks), 0) == slot.astype(jnp.int32)
    ).astype(BF16)
    selt[...] = (
        lax.broadcasted_iota(jnp.int32, (toks, slots), 1) == slot_col.astype(jnp.int32)
    ).astype(BF16)
    names = lax.broadcasted_iota(jnp.int32, (experts, toks), 0)
    by_expert = jnp.zeros((experts, toks), F32)
    for k in range(route_ref.shape[0]):
        by_expert = by_expert + jnp.where(
            names == route_ref[k : k + 1, :], rw_ref[k : k + 1, :], 0.0
        )
    by_slot = exact_pick(by_expert, selt[...])
    table = by_slot[:, 0:cap]
    for g in range(1, GROUPS):
        table = table + by_slot[:, g * cap : (g + 1) * cap]
    meta[sp, 0:experts, :] = table

    @pl.when(c == 1)
    def _():
        kv_sib_copy(2 * z).wait_recv()
        process(2 * z, False)

    def give_credits(j):
        def credit(which, plane):
            pl.semaphore_signal(
                free_sem.at[which], inc=1, device_id={"sp": 2 * plane + c, "tp": tp},
                device_id_type=MESH,
            )

        @pl.when(jnp.logical_and(j == z, z == zs - 2))
        def _():
            credit(0, 0)

        @pl.when(jnp.logical_and(j == z, z == zs - 1))
        def _():
            credit(1, 0)
            credit(1, 1)

    def visit(j, carry):
        b = 2 * (z - j) + c
        other = 2 * (z - j) + 1 - c
        with SC('wait_b'):
            kv_sib_copy(b).wait_recv()

        @pl.when(z < zs - 1)
        def _():
            next_copy(b).start()

        kv_sib_copy(b).start()
        give_credits(j)
        with SC('proc_b'):
            process(b, False)
        with SC('wait_o'):
            kv_sib_copy(other).wait_recv()
        with SC('proc_o'):
            process(other, False)
        return carry

    lax.fori_loop(1, z + 1, visit, 0)

    for h in range(heads):
        blend = acc[h] * (1.0 / totals[h])
        mix = blend[:, :toks] - lam_ref[h] * blend[:, toks:]
        mix = mix * lax.rsqrt(jnp.mean(mix * mix, axis=0, keepdims=True) + norm_eps)
        att[:, h * head_width : (h + 1) * head_width] = (mix.T * gain_ref[...]).astype(BF16)
    inputs[3].wait()

    def projected(to):
        return jnp.dot(
            att[...], owv[:, pl.ds(pl.multiple_of(to * piece, piece), piece)],
            preferred_element_type=F32,
        )

    half_toks = toks // 2
    part_halves = (slice(0, half_toks), slice(half_toks, toks))

    def rs_copy(i):
        to, source, target = [
            (beside, part.at[across, part_halves[0]], ppass.at[0]),
            (above, part.at[across, part_halves[1]], ppass.at[1]),
            (beside, part.at[beside, part_halves[0]], rbuf.at[0, part_halves[0]]),
            (above, part.at[above, part_halves[1]], rbuf.at[1, part_halves[1]]),
            (above, part.at[above, part_halves[0]], rbuf.at[1, part_halves[0]]),
            (beside, part.at[beside, part_halves[1]], rbuf.at[0, part_halves[1]]),
        ][i]
        return remote(source, target, rs_send, rs_recv.at[min(i, 2)], sp, to)

    part[across] = projected(across).astype(BF16)
    rs_copy(0).start()
    rs_copy(1).start()
    for_beside = projected(beside)
    part[beside, part_halves[0]] = for_beside[part_halves[0]].astype(BF16)
    rs_copy(2).start()
    for_above = projected(above)
    part[above, part_halves[1]] = for_above[part_halves[1]].astype(BF16)
    rs_copy(3).start()
    mine = pl.ds(pl.multiple_of(tp * piece, piece), piece)
    inputs[4].wait()
    total = resv[:, mine].astype(F32) + projected(tp)
    with SC("rs_pass"):
        rs_copy(0).wait_recv()
    part[above, part_halves[0]] = (for_above[part_halves[0]] + ppass[0].astype(F32)).astype(BF16)
    rs_copy(4).start()
    with SC("rs_pass"):
        rs_copy(1).wait_recv()
    part[beside, part_halves[1]] = (for_beside[part_halves[1]] + ppass[1].astype(F32)).astype(BF16)
    rs_copy(5).start()
    wd_start(2)

    half_cap = cap // 2

    def spot(src, core, part):
        return xall.at[
            src,
            pl.ds(pl.multiple_of(core * cap, cap), cap),
            pl.ds(pl.multiple_of(part * piece, piece), piece),
        ]

    def half_spot(src, part, side):
        return xall.at[
            src,
            pl.ds(pl.multiple_of(c * cap + side * half_cap, half_cap), half_cap),
            pl.ds(pl.multiple_of(part * piece, piece), piece),
        ]

    def x_copy(s):
        group = (z + s) % zs
        return remote(
            xs.at[s], spot(z, c, tp), x_send, x_recv.at[z, 0], 2 * group + c, tp
        )

    def spot_wait(here, sem):
        remote(here, here, x_send, sem, sib, tp).wait_recv()

    def tp_copy(src, i):
        to, side = [(beside, 0), (above, 1), (beside, 1), (above, 0)][i]
        here = half_spot(src, tp, side)
        return remote(here, here, x_tp, x_recv.at[src, 1 + i], sp, to)

    def pass_copy(src, i):
        part, side, to = [(beside, 0, above), (above, 1, beside)][i]
        here = half_spot(src, part, side)
        return remote(here, here, x_tp, x_recv.at[src, 5], sp, to)

    def sib_copy(src, part):
        here = spot(src, c, part)
        return remote(here, here, x_sib, s_recv.at[src], sib, tp)

    def gather(src):
        @pl.when(src != z)
        def _():
            with SC("arrive"):
                spot_wait(spot(src, c, tp), x_recv.at[src, 0])

        for i in range(4):
            tp_copy(src, i).start()
        sib_copy(src, tp).start()

    def gather_pass(src):
        with SC("gpass"):
            spot_wait(half_spot(src, beside, 0), x_recv.at[src, 1])
        pass_copy(src, 0).start()
        with SC("gpass"):
            spot_wait(half_spot(src, above, 1), x_recv.at[src, 2])
        pass_copy(src, 1).start()

    def forward(src):
        with SC("compl_tp"):
            spot_wait(half_spot(src, beside, 1), x_recv.at[src, 3])
            sib_copy(src, beside).start()
            spot_wait(half_spot(src, above, 0), x_recv.at[src, 4])
            sib_copy(src, above).start()
            spot_wait(spot(src, c, across), x_recv.at[src, 5])
            sib_copy(src, across).start()

    def complete(src):
        with SC("compl_sib"):
            spot_wait(
                xall.at[src, pl.ds(pl.multiple_of((1 - c) * cap, cap), cap)], s_recv.at[src]
            )

    pl.when(z > 0)(lambda: gather(0))
    pl.when(z == zs - 2)(lambda: gather(1))

    with SC("rs_wait"):
        remote(rbuf, rbuf, rs_send, rs_recv.at[2], sp, beside).wait_recv()
    total = total + rbuf[0].astype(F32) + rbuf[1].astype(F32)
    stream_ref[...] = total
    normed_ref[...] = (total * fg_ref[:, mine]).astype(BF16)
    squares = jnp.sum(total * total, axis=1, keepdims=True)
    as_row = jnp.sum(jnp.where(eye, squares, 0.0), axis=0, keepdims=True)
    sq_send[...] = jnp.broadcast_to(as_row, sq_send.shape)

    def sq_copy(d):
        return remote(
            sq_send, sq_recv.at[d], sq_ss, sq_rs, sp, (tp + d) % tps
        )

    for d in range(1, tps):
        sq_copy(d).start()

    def m_copy(d):
        return remote(meta.at[sp], meta.at[sp], m_send, m_recv.at[sp], (sp + d) % n, tp)

    def m_wait(src):
        @pl.when(src != sp)
        def _():
            remote(meta.at[src], meta.at[src], m_send, m_recv.at[src], sib, tp).wait_recv()

    for s in list(range(1, zs)) + [0]:
        group = (z + s) % zs
        picked = jnp.dot(
            sel[pl.ds(pl.multiple_of(group * cap, cap), cap), :], normed_ref[...],
            preferred_element_type=F32,
        ).astype(BF16)
        if s:
            xs[s] = picked
            pl.when(z >= (zs - s if s >= zs - 2 else 0))(lambda: x_copy(s).start())
        else:
            spot(z, c, tp)[...] = picked

    @pl.when(z < zs - 1)
    def _():
        gather(z)

    wd_start(3)

    def row_factors():
        with SC("sq_wait"):
            squares_in = sq_recv.at[pl.ds(1, tps - 1)]
            remote(squares_in, squares_in, sq_ss, sq_rs, sp, beside).wait_recv()
        sums = sq_send[0:1, :]
        for d in range(1, tps):
            sums = sums + sq_recv[d, 0:1, :]
        inverse = lax.rsqrt(sums * (1.0 / (piece * tps)) + norm_eps)
        by_slot = exact_pick(jnp.broadcast_to(inverse, (8, toks)), selt[...])
        for g in range(GROUPS):
            meta[sp, experts + g : experts + g + 1, :] = by_slot[0:1, g * cap : (g + 1) * cap]
        for d in range(1, n):
            m_copy(d).start()

    def late_rows(s, which):
        with SC("credit"):
            pl.semaphore_wait(free_sem.at[which], 1)
        x_copy(s).start()

    pl.when(z < zs - 2)(row_factors)
    gather_pass(0)

    @pl.when(z == zs - 2)
    def _():
        gather_pass(1)
        gather_pass(2)

    pl.when(z == zs - 1)(lambda: gather(1))
    wd_start(4)
    pl.when(z == zs - 2)(row_factors)
    pl.when(z == 1)(lambda: late_rows(zs - 2, 1))

    @pl.when(z == 0)
    def _():
        late_rows(zs - 2, 0)
        gather(1)
        late_rows(zs - 1, 1)

    def late_sources():
        gather(zs - 2)
        pl.when(z == 0)(lambda: gather_pass(1))
        wd_start(5)
        forward(1)
        gather_pass(zs - 2)
        wd_start(6)

    def near_copy(src, part):
        return remote(
            away.at[src, part], near.at[src, part], n_send,
            n_recv.at[src, jnp.where(part == across, 0, 1)], sib, tp,
        )

    def near_wait(src, first):
        here = near.at[src, pl.ds(0, 1 if first else tps - 1)]
        remote(here, here, n_send, n_recv.at[src, 0 if first else 1], sib, tp).wait_recv()

    tile = 256
    small_eye = lax.broadcasted_iota(jnp.int32, (cap, cap), 0) == lax.broadcasted_iota(
        jnp.int32, (cap, cap), 1
    )
    which = lax.broadcasted_iota(jnp.int32, meta.shape[1:], 0)

    def meta_col(src, core, line):
        row = jnp.sum(jnp.where(which == line, meta[2 * src + core], 0.0), axis=0, keepdims=True)
        return jnp.sum(jnp.where(small_eye, row, 0.0), axis=1, keepdims=True)

    keep_rows = pl.ds(pl.multiple_of(c * cap, cap), cap)
    away_rows = pl.ds(pl.multiple_of((1 - c) * cap, cap), cap)

    def ffn_one(src, between):
        @pl.when(src == 0)
        def _():
            for load in loads:
                load.wait()

        with SC("m_wait"):
            m_wait(2 * src)
            m_wait(2 * src + 1)
        factor = jnp.concatenate(
            [meta_col(src, c, experts + z), meta_col(src, 1 - c, experts + z)], axis=0
        )

        def one(i, carry):
            pl.when(i == wg.shape[1] // tile // 2)(between)
            at = pl.ds(pl.multiple_of(i * tile, tile), tile)
            x = jnp.concatenate([xall[src, keep_rows], xall[src, away_rows]], axis=0)
            gate = jnp.dot(x, wg[:, at], preferred_element_type=F32) * factor
            up = jnp.dot(x, wu[:, at], preferred_element_type=F32) * factor
            hid[src, :, at] = (gate / (1.0 + jnp.exp(-gate)) * up).astype(BF16)
            return carry

        with SC("ffn_one"):
            lax.fori_loop(0, wg.shape[1] // tile, one, 0)

    def ffn_two(src):
        @pl.when(src == 0)
        def _():
            with SC("down_wait"):
                others = wdv.at[pl.ds(0, tps - 1)]
                remote(others, others, wd_send, wd_recv, sp, beside).wait()

        row_weight = jnp.concatenate(
            [meta_col(src, c, sp), meta_col(src, 1 - c, sp)], axis=0
        )

        def two(j, carry):
            to = tp ^ (tps - 1 - j)
            result = jnp.dot(hid[src], wdv[to], preferred_element_type=F32) * row_weight
            away[src, to] = result[cap:].astype(BF16)
            near_copy(src, to).start()
            keep[src, to] = result[:cap]
            return carry

        with SC("ffn_two"):
            lax.fori_loop(0, tps, two, 0)

    cap_halves = (slice(0, half_cap), slice(half_cap, cap))

    def r_copy(src, i):
        to, source, target = [
            (beside, rsend.at[src, across, cap_halves[0]], rpass.at[src, 0]),
            (above, rsend.at[src, across, cap_halves[1]], rpass.at[src, 1]),
            (beside, rsend.at[src, beside, cap_halves[0]], rrecv.at[src, 0, cap_halves[0]]),
            (above, rsend.at[src, above, cap_halves[1]], rrecv.at[src, 1, cap_halves[1]]),
            (above, rsend.at[src, above, cap_halves[0]], rrecv.at[src, 1, cap_halves[0]]),
            (beside, rsend.at[src, beside, cap_halves[1]], rrecv.at[src, 0, cap_halves[1]]),
        ][i]
        return remote(source, target, r_send, r_recv.at[src, min(i, 2)], sp, to)

    def both(src, to, at):
        return keep[src, to, at, :] + near[src, to, at, :].astype(F32)

    def spread(src):
        with SC("near_wait"):
            near_wait(src, True)
        rsend[src, across] = both(src, across, slice(0, cap)).astype(BF16)
        r_copy(src, 0).start()
        r_copy(src, 1).start()
        near_wait(src, False)
        rsend[src, above, cap_halves[1]] = both(src, above, cap_halves[1]).astype(BF16)
        r_copy(src, 3).start()
        rsend[src, beside, cap_halves[0]] = both(src, beside, cap_halves[0]).astype(BF16)
        r_copy(src, 2).start()

    def spread_pass(src):
        with SC("spass"):
            r_copy(src, 0).wait_recv()
        rsend[src, above, cap_halves[0]] = (
            both(src, above, cap_halves[0]) + rpass[src, 0].astype(F32)
        ).astype(BF16)
        r_copy(src, 4).start()
        with SC("spass"):
            r_copy(src, 1).wait_recv()
        rsend[src, beside, cap_halves[1]] = (
            both(src, beside, cap_halves[1]) + rpass[src, 1].astype(F32)
        ).astype(BF16)
        r_copy(src, 5).start()

    def b_copy(src):
        return remote(
            back.at[src], ret.at[z], b_send, b_recv, 2 * src + c, tp
        )

    def finish(src):
        with SC("r_wait"):
            here = rrecv.at[src]
            remote(here, here, r_send, r_recv.at[src, 2], sp, beside).wait_recv()
        total = both(src, tp, slice(0, cap))
        total = total + rrecv[src, 0].astype(F32) + rrecv[src, 1].astype(F32)

        @pl.when(src == z)
        def _():
            ret[z] = total.astype(BF16)

        @pl.when(src != z)
        def _():
            back[src] = total.astype(BF16)
            b_copy(src).start()

    last = zs - 1

    at_last = z == last

    early = z < last

    def when_both(one, two):
        return pl.when(jnp.logical_and(one, two))

    third = z == last - 1
    first_two = z < last - 1

    def up_step(s):
        def between():
            when_both(third, s == 0)(lambda: forward(1))
            when_both(z == 1, s == 0)(lambda: gather_pass(1))
            when_both(early, s == 1)(lambda: forward(2))
            when_both(early, s == last - 1)(lambda: gather(last))
            when_both(third, s == last)(lambda: spread_pass(1))
            when_both(at_last, s < last)(lambda: gather_pass(s + 1))
            when_both(at_last, s + 2 <= last)(lambda: gather(s + 2))

        pl.when(s == 0)(lambda: forward(0))
        when_both(first_two, s == 1)(late_sources)
        complete(s)
        ffn_one(s, between)
        when_both(z != last - 1, s == last)(lambda: spread_pass(last - 1))
        when_both(early, s == last)(lambda: finish(0))
        when_both(first_two, s == last)(lambda: finish(1))

    def down_step(s):
        ffn_two(s)
        when_both(at_last, s < last)(lambda: forward(s + 1))
        when_both(s >= 1, jnp.where(third, s == 1, s < last))(lambda: spread_pass(s - 1))
        when_both(third, s == last - 1)(lambda: spread_pass(last))
        spread(s)
        when_both(early, s == 0)(lambda: gather_pass(last))
        pl.when(jnp.where(third, s == 1, jnp.logical_and(first_two, s == last - 1)))(
            lambda: forward(last)
        )
        when_both(at_last, s == 0)(row_factors)
        when_both(at_last, s == last - 1)(lambda: finish(0))
        when_both(z >= last - 1, s == last)(lambda: finish(1))
        when_both(z != last - 1, s == last)(lambda: finish(2))

    def step(k, carry):
        turn = k
        for at, (one, two) in enumerate(
            ((0, 0), (2, 2), (4, 4), (1, 1), (3, 3), (5, 6), (6, 7), (7, 5))
        ):
            turn = jnp.where(jnp.logical_and(first_two, k == at), one, turn)
            turn = jnp.where(jnp.logical_and(third, k == at), two, turn)
        pl.when(turn % 2 == 0)(lambda: up_step(turn // 2))
        pl.when(turn % 2 == 1)(lambda: down_step(turn // 2))
        return carry

    lax.fori_loop(0, 2 * zs, step, 0)
    pl.when(z != last - 1)(lambda: spread_pass(last))
    pl.when(third)(lambda: spread_pass(last - 1))
    finish(last)
    pl.when(third)(lambda: finish(last - 1))

    with SC("b_wait"):
        returns = ret.at[pl.ds(0, zs - 1)]
        remote(returns, returns, b_send, b_recv, sib, tp).wait_recv()
    rows = ret[...].reshape(zs * cap, piece)
    layer = stream_ref[...] + jnp.dot(selt[...], rows, preferred_element_type=F32)
    outv[:, mine] = layer.astype(BF16)

    def out_spot(part, side):
        return outv.at[part_halves[side], pl.ds(pl.multiple_of(part * piece, piece), piece)]

    def o_copy(i):
        part, side, to = [
            (tp, 0, beside), (tp, 1, above), (tp, 1, beside), (tp, 0, above),
            (beside, 0, above), (above, 1, beside),
        ][i]
        here = out_spot(part, side)
        return remote(here, here, o_send, o_recv.at[min(i, 4)], sp, to)

    def o_wait(part, i, side=None):
        at = pl.ds(pl.multiple_of(part * piece, piece), piece)
        here = outv.at[:, at] if side is None else out_spot(part, side)
        remote(here, here, o_send, o_recv.at[i], sib, tp).wait_recv()

    for i in range(4):
        o_copy(i).start()
    with SC("o_pass"):
        o_wait(beside, 0, 0)
    o_copy(4).start()
    with SC("o_pass"):
        o_wait(above, 1, 1)
    o_copy(5).start()

    def sent(here, sem):
        remote(here, here, sem, kv_recv.at[0], sib, tp).wait_send()

    sent(sq_recv.at[pl.ds(1, tps - 1)], sq_ss)
    sent(part.at[pl.ds(0, 3)], rs_send)
    sent(meta.at[pl.ds(0, n - 1)], m_send)
    sent(xs.at[pl.ds(1, zs - 1)], x_send)
    sent(back.at[pl.ds(0, zs - 1)], b_send)
    sent(away, n_send)
    sent(away, x_sib)
    sent(away.at[pl.ds(0, zs - 1)], x_tp)
    sent(away.at[pl.ds(0, zs - 1)], r_send)

    @pl.when(z < zs - 1)
    def _():
        next_copy(sp).wait_send()

    @pl.when(c == 0)
    def _():
        kv_sib_copy(sp).wait_send()

    def drain(j, carry):
        b = 2 * (z - j) + c

        @pl.when(z < zs - 1)
        def _():
            next_copy(b).wait_send()

        kv_sib_copy(b).wait_send()
        return carry

    lax.fori_loop(1, z + 1, drain, 0)
    with SC("o_wait"):
        o_wait(beside, 2, 1)
        o_wait(above, 3, 0)
        o_wait(across, 4)
    with SC("o_send"):
        sent(part.at[pl.ds(0, 3)], o_send)


def paired_shards(
    residual, queries, key_vectors, value_rows, head_lambda, head_gain, out_weight, ffn_gain,
    expert_gate, expert_up, expert_down, routing, route_weight,
):
    n = lax.axis_size("sp")
    tps = lax.axis_size("tp")
    toks, heads, head_width = queries.shape
    width = heads * head_width
    model = residual.shape[1]
    piece = model // tps
    experts = n
    per_group = experts // GROUPS
    cap = toks // per_group
    down = expert_down[0]
    wd_rows = down.shape[0] // tps
    vmem = pl.BlockSpec(memory_space=pltpu.VMEM)
    smem = pl.BlockSpec(memory_space=pltpu.SMEM)
    hbm = pl.BlockSpec(memory_space=pltpu.HBM)
    dma = pltpu.SemaphoreType.DMA
    zs = n // 2
    def stay(x):
        return pltpu.with_memory_space_constraint(x, pltpu.HBM)

    return pl.pallas_call(
        functools.partial(layer_kernel, n, tps, cap, heads, head_width),
        out_shape=jax.ShapeDtypeStruct((toks, model), BF16),
        in_specs=[hbm, hbm, hbm, vmem, vmem, hbm, smem, vmem, hbm, hbm, vmem, hbm, hbm],
        out_specs=vmem,
        scratch_shapes=[
            pltpu.VMEM((3, toks * heads, head_width), BF16),
            pltpu.VMEM((toks, model), BF16),
            pltpu.VMEM((width, model), BF16),
            pltpu.VMEM((GROUPS * cap, toks), BF16),
            pltpu.VMEM((toks, GROUPS * cap), BF16),
            pltpu.VMEM((toks, piece), F32),
            pltpu.VMEM((toks, piece), BF16),
            pltpu.VMEM((n, experts + 8, cap), F32),
            pltpu.VMEM((zs, cap, piece), BF16),
            pltpu.VMEM((zs, 2 * cap, model), BF16),
            pltpu.VMEM(expert_gate.shape[1:], BF16),
            pltpu.VMEM(expert_up.shape[1:], BF16),
            pltpu.VMEM((tps, wd_rows, piece), BF16),
            pltpu.VMEM((zs, 2 * cap, expert_gate.shape[2]), BF16),
            pltpu.VMEM((zs, tps, cap, piece), F32),
            pltpu.VMEM((zs, tps, cap, piece), BF16),
            pltpu.VMEM((zs, tps, cap, piece), BF16),
            pltpu.VMEM((zs, tps, cap, piece), BF16),
            pltpu.VMEM((zs, 2, cap, piece), BF16),
            pltpu.VMEM((zs, 2, cap // 2, piece), BF16),
            pltpu.VMEM((zs, cap, piece), BF16),
            pltpu.VMEM((zs, cap, piece), BF16),
            pltpu.VMEM((n, heads * toks, head_width), BF16),
            pltpu.VMEM((n, width, toks), BF16),
            pltpu.VMEM((heads * toks, head_width), BF16),
            pltpu.VMEM((heads, head_width, 2 * toks), BF16),
            pltpu.VMEM((heads, 1, 2 * toks), F32),
            pltpu.VMEM((heads, 1, 2 * toks), F32),
            pltpu.VMEM((heads, head_width, 2 * toks), F32),
            pltpu.VMEM((toks, width), BF16),
            pltpu.VMEM((tps, toks, piece), BF16),
            pltpu.VMEM((2, toks, piece), BF16),
            pltpu.VMEM((2, toks // 2, piece), BF16),
            pltpu.VMEM((8, toks), F32),
            pltpu.VMEM((tps, 8, toks), F32),
            dma((5,)), dma((3,)),
            dma, dma, dma, dma((zs, 6)), dma((zs,)),
            dma, dma((zs, 2)), dma, dma((zs, 3)),
            dma, dma, dma, dma((5,)),
            dma((n,)), dma((n,)), dma((n,)),
            dma, dma, dma, dma((n,)),
            dma, dma((3,)), dma, dma, pltpu.SemaphoreType.REGULAR((2,)),
        ],
        compiler_params=pltpu.CompilerParams(collective_id=0, has_side_effects=True, vmem_limit_bytes=49545216),
        name="layer",
    )(
        stay(queries.reshape(toks * heads, head_width)), stay(key_vectors.reshape(toks * heads, head_width)),
        stay(value_rows.reshape(toks * heads, head_width)), stay(routing.T), stay(route_weight.T), stay(down),
        stay(head_lambda), stay(head_gain.reshape(1, -1)), stay(out_weight), stay(residual), stay(ffn_gain.reshape(1, -1)),
        stay(expert_gate), stay(expert_up),
    )


def solution(mesh):
    in_specs = (
        P("sp", None),
        P("sp", "tp", None),
        P("sp", "tp", None),
        P("sp", "tp", None),
        P("tp"),
        P(),
        P("tp", None),
        P(),
        P("sp", None, "tp"),
        P("sp", None, "tp"),
        P("sp", None, "tp"),
        P("sp", None),
        P("sp", None),
    )
    out_specs = P("sp", None)
    paired = mesh.shape["sp"] == 2 * GROUPS and mesh.shape["tp"] == 4
    return jax.shard_map(paired_shards if paired else shards, mesh=mesh, in_specs=in_specs, out_specs=out_specs, check_vma=False)
```

```python
import functools
import math

import jax
import jax.numpy as jnp
from jax import lax
from jax.experimental import pallas as pl
from jax.experimental.pallas import tpu as pltpu
from jax.sharding import PartitionSpec as P

GROUPS = 4
SC = jax.named_scope


norm_eps = 1e-06


def online_update(running, query_part, key_part, value_part, query_pos, key_pos, score_scale):
    highest, totals, accum = running
    scores = (
        jnp.einsum("qhd,khd->hqk", query_part, key_part, preferred_element_type=jnp.float32)
        * score_scale
    )
    scores = jnp.where(key_pos[None, None, :] <= query_pos[None, :, None], scores, -jnp.inf)
    new_high = jnp.maximum(highest, jnp.max(scores, axis=-1))
    shrink = jnp.exp(highest - new_high)
    weights = jnp.exp(scores - new_high[:, :, None])
    totals = shrink * totals + jnp.sum(weights, axis=-1)
    blended = jnp.einsum(
        "hqk,khe->qhe", weights.astype(jnp.bfloat16), value_part, preferred_element_type=jnp.float32
    )
    accum = jnp.transpose(shrink)[:, :, None] * accum + blended
    return (new_high, totals, accum)


def shards(
    residual,
    queries,
    key_vectors,
    value_rows,
    head_lambda,
    head_gain,
    out_weight,
    ffn_gain,
    expert_gate,
    expert_up,
    expert_down,
    routing,
    route_weight,
):
    tok_count = queries.shape[0]
    local_heads = queries.shape[1]
    half_width = queries.shape[2] // 2
    value_width = value_rows.shape[2]
    score_scale = half_width ** (-0.5)
    query_pos = lax.axis_index("sp") * tok_count + jnp.arange(tok_count, dtype=jnp.int32)
    last_query = query_pos[-1]
    first_half = queries[:, :, :half_width]
    second_half = queries[:, :, half_width:]
    start_high = jnp.full((local_heads, tok_count), -1e30, jnp.float32)
    start_total = jnp.zeros((local_heads, tok_count), jnp.float32)
    start_accum = jnp.zeros((tok_count, local_heads, value_width), jnp.float32)
    empty_state = (start_high, start_total, start_accum)
    running = (empty_state, empty_state)
    key_piece = lax.all_gather(key_vectors, "sp", axis=0, tiled=True)
    value_piece = lax.all_gather(value_rows, "sp", axis=0, tiled=True)
    piece_len = key_piece.shape[0]
    block_len = math.gcd(piece_len, 512)
    block_count = piece_len // block_len
    key_blocks = key_piece.reshape(block_count, block_len, local_heads, 2 * half_width)
    value_blocks = value_piece.reshape(block_count, block_len, local_heads, value_width)

    def visit(current, stacked):
        block_index, key_block, value_block = stacked
        block_first = block_index * block_len
        key_pos = block_first + jnp.arange(block_len, dtype=jnp.int32)

        def compute(inside):
            first_state = online_update(
                inside[0],
                first_half,
                key_block[:, :, :half_width],
                value_block,
                query_pos,
                key_pos,
                score_scale,
            )
            second_state = online_update(
                inside[1],
                second_half,
                key_block[:, :, half_width:],
                value_block,
                query_pos,
                key_pos,
                score_scale,
            )
            return (first_state, second_state)

        return (lax.cond(block_first <= last_query, compute, lambda inside: inside, current), None)

    running, _ = lax.scan(
        visit, running, (jnp.arange(block_count, dtype=jnp.int32), key_blocks, value_blocks)
    )
    first_state, second_state = running
    first_out = first_state[2] / jnp.transpose(first_state[1])[:, :, None]
    second_out = second_state[2] / jnp.transpose(second_state[1])[:, :, None]
    combined = first_out - head_lambda[None, :, None] * second_out
    normed_heads = (
        combined
        * lax.rsqrt(jnp.mean(combined * combined, axis=-1, keepdims=True) + norm_eps)
        * head_gain
    )
    attended = normed_heads.astype(jnp.bfloat16).reshape(tok_count, local_heads * value_width)
    partial_proj = jnp.dot(attended, out_weight, preferred_element_type=jnp.float32)
    projected = lax.psum(partial_proj.astype(jnp.bfloat16), "tp").astype(jnp.float32)
    stream = residual.astype(jnp.float32) + projected
    block_normed = (
        stream * lax.rsqrt(jnp.mean(stream * stream, axis=-1, keepdims=True) + norm_eps) * ffn_gain
    ).astype(jnp.bfloat16)
    expert_count = lax.axis_size("sp")
    tp_count = lax.axis_size("tp")
    per_group = expert_count // GROUPS
    capacity = tok_count // per_group
    top_count = routing.shape[1]
    model_width = block_normed.shape[1]
    flat_routes = routing.reshape(-1)
    route_count = flat_routes.shape[0]
    onehot = (flat_routes[:, None] == jnp.arange(expert_count, dtype=jnp.int32)[None, :]).astype(
        jnp.int32
    )
    earlier = jnp.cumsum(onehot, axis=0) - onehot
    position = jnp.sum(earlier * onehot, axis=1)
    slot_index = flat_routes * capacity + position
    slot_token = (
        jnp.full((expert_count * capacity,), tok_count, jnp.int32)
        .at[slot_index]
        .set(jnp.arange(route_count, dtype=jnp.int32) // top_count)
    )
    slot_table = slot_token.reshape(expert_count, capacity)
    slice_width = model_width // tp_count
    own_columns = lax.dynamic_slice_in_dim(
        block_normed, lax.axis_index("tp") * slice_width, slice_width, 1
    )
    outgoing = jnp.take(own_columns, slot_table, axis=0, mode="fill", fill_value=0)
    landed = lax.all_to_all(outgoing, "sp", split_axis=0, concat_axis=0, tiled=True)
    arrived = lax.all_gather(landed, "tp", axis=2, tiled=True)
    expert_rows = arrived.reshape(-1, model_width)
    gate_part = jnp.dot(expert_rows, expert_gate[0], preferred_element_type=jnp.float32)
    up_part = jnp.dot(expert_rows, expert_up[0], preferred_element_type=jnp.float32)
    inner_act = (jax.nn.silu(gate_part) * up_part).astype(jnp.bfloat16)
    down_width = expert_down.shape[2]
    weight_rows = expert_down[0]
    expert_sum = jnp.dot(
        lax.all_gather(inner_act, "tp", axis=1, tiled=True),
        weight_rows,
        preferred_element_type=jnp.float32,
    )
    expert_out = expert_sum.astype(jnp.bfloat16).reshape(expert_count, capacity, down_width)
    returned = lax.all_to_all(expert_out, "sp", split_axis=0, concat_axis=0, tiled=True)
    per_route = returned.reshape(expert_count * capacity, down_width)[slot_index]
    weighted = per_route.astype(jnp.float32) * route_weight.reshape(-1)[:, None]
    token_sum = jnp.sum(weighted.reshape(tok_count, top_count, down_width), axis=1)
    moe_rows = lax.all_gather(token_sum.astype(jnp.bfloat16), "tp", axis=1, tiled=True).astype(
        token_sum.dtype
    )
    return (stream + moe_rows).astype(jnp.bfloat16)


MESH = pl.DeviceIdType.MESH
F32 = jnp.float32
BF16 = jnp.bfloat16


def remote(src, dst, send_sem, recv_sem, sp, tp):
    return pltpu.make_async_remote_copy(
        src_ref=src,
        dst_ref=dst,
        send_sem=send_sem,
        recv_sem=recv_sem,
        device_id={"sp": sp, "tp": tp},
        device_id_type=MESH,
    )


def mixed_dot(left, right, contract):
    return lax.dot_general(left, right, (contract, ((), ())), preferred_element_type=F32)


def dispersed(value):
    high = value.astype(BF16)
    rest = value - high.astype(F32)
    middle = rest.astype(BF16)
    low = (rest - middle.astype(F32)).astype(BF16)
    return jnp.concatenate([high, middle, low], axis=0)


def exact_pick(value, picker):
    count = value.shape[0]
    parts = mixed_dot(dispersed(value), picker, ((1,), (0,)))
    return parts[:count] + parts[count : 2 * count] + parts[2 * count :]


def layer_kernel(
    n, tps, cap, heads, head_width,
    q_ref, k_ref, v_ref, route_in, rw_in, wd_ref, lam_in, gain_in, ow_ref, res_ref, fg_in,
    gate_ref, up_ref,
    outv,
    route_ref, rw_ref, lam_ref, gain_ref, fg_ref, raw, resv, owv, sel, selt, stream_ref, normed_ref, meta,
    xs, xall, wg, wu, wdv, hid, keep, away, near, rsend, rrecv, rpass, back, ret,
    kall, vall, rowm, qs, highs, totals, acc, att, part, rbuf, ppass, sq_send, sq_recv,
    in_sem, w_sem, x_send, x_tp, x_sib, x_recv, s_recv, n_send, n_recv, r_send, r_recv,
    b_send, b_recv, o_send, o_recv,
    kv_next, kv_sib, kv_recv, wd_send, wd_recv, m_send, m_recv,
    rs_send, rs_recv, sq_ss, sq_rs, free_sem,
):
    sp = lax.axis_index("sp")
    tp = lax.axis_index("tp")
    z, c = sp // 2, sp % 2
    zs = n // 2
    sib = 2 * z + 1 - c
    toks = resv.shape[0]
    width = heads * head_width
    half = head_width // 2
    piece = normed_ref.shape[1]
    wd_rows = wdv.shape[1]
    experts = n
    per_group = experts // GROUPS
    beside, above, across = tp ^ 1, tp ^ 2, tp ^ 3

    barrier = pltpu.get_barrier_semaphore()
    for d in range(1, n):
        pl.semaphore_signal(
            barrier, inc=1, device_id={"sp": (sp + d) % n, "tp": tp}, device_id_type=MESH
        )
    for d in range(1, tps):
        pl.semaphore_signal(
            barrier, inc=1, device_id={"sp": sp, "tp": (tp + d) % tps}, device_id_type=MESH
        )
    inputs = [
        pltpu.make_async_copy(k_ref, raw.at[0], in_sem.at[0]),
        pltpu.make_async_copy(v_ref, raw.at[1], in_sem.at[1]),
        pltpu.make_async_copy(q_ref, raw.at[2], in_sem.at[2]),
        pltpu.make_async_copy(ow_ref, owv, in_sem.at[3]),
        pltpu.make_async_copy(res_ref, resv, in_sem.at[4]),
    ]
    small = [
        pltpu.make_async_copy(given, kept, in_sem.at[5 + i])
        for i, (given, kept) in enumerate(
            (
                (route_in, route_ref), (rw_in, rw_ref), (lam_in, lam_ref), (gain_in, gain_ref),
                (fg_in, fg_ref),
            )
        )
    ]
    loads = [
        pltpu.make_async_copy(gate_ref.at[0], wg, w_sem.at[0]),
        pltpu.make_async_copy(up_ref.at[0], wu, w_sem.at[1]),
        pltpu.make_async_copy(
            wd_ref.at[pl.ds(pl.multiple_of(tp * wd_rows, wd_rows), wd_rows), :],
            wdv.at[tp], w_sem.at[2],
        ),
    ]
    for load in inputs + small + loads:
        load.start()

    run = toks // heads
    spot_row = lax.broadcasted_iota(jnp.int32, (run, toks), 0)
    spot_col = lax.broadcasted_iota(jnp.int32, (run, toks), 1)
    order = jnp.concatenate(
        [(spot_col == spot_row * heads + h).astype(BF16) for h in range(heads)], axis=0
    )

    def split(which, store):
        for i in range(heads):
            rows = jnp.dot(
                order, raw[which, i * toks : (i + 1) * toks, :], preferred_element_type=F32
            )
            for h in range(heads):
                store(i, h, rows[h * run : (h + 1) * run, :])

    def head_rows(h, i=0, count=toks):
        return slice(h * toks + i * run, h * toks + i * run + count)

    def store_keys(i, h, rows):
        kall[sp, head_rows(h, i, run), :] = rows.astype(BF16)

    def store_rows(i, h, rows):
        rowm[head_rows(h, i, run), :] = rows.astype(BF16)

    unit = (
        lax.broadcasted_iota(jnp.int32, (head_width, head_width), 0)
        == lax.broadcasted_iota(jnp.int32, (head_width, head_width), 1)
    ).astype(BF16)

    def turned(h):
        return mixed_dot(unit, rowm[head_rows(h), :], ((1,), (1,)))

    inputs[0].wait()
    split(0, store_keys)
    inputs[1].wait()
    split(1, store_rows)
    for h in range(heads):
        vall[sp, h * head_width : (h + 1) * head_width, :] = turned(h).astype(BF16)

    chunks = 8
    wd_run = wd_rows // chunks

    def wd_copy(k, d):
        to = tp ^ d
        return remote(
            wd_ref.at[pl.ds(pl.multiple_of(to * wd_rows + k * wd_run, wd_run), wd_run), :],
            wdv.at[tp, pl.ds(pl.multiple_of(k * wd_run, wd_run), wd_run)],
            wd_send, wd_recv, sp, to,
        )

    def by_plane(values):
        chosen = values[-1]
        for plane, value in enumerate(values[:-1]):
            chosen = jnp.where(z == plane, value, chosen)
        return chosen

    wd_points = [
        (0, 0, 0, 0), (1, 3, 5, 7), (2, 4, 6, 7), (3, 4, 6, 7), (6, 6, 8, 8), (7, 7, 8, 8), (8, 8, 8, 8)
    ]

    def wd_start(point):
        def start(k, carry):
            for d in (3, 1, 2):
                wd_copy(k, d).start()
            return carry

        lax.fori_loop(by_plane(wd_points[point - 1]), by_plane(wd_points[point]), start, 0)

    class KeyCopies:
        def __init__(self, b, sends, to):
            self.at = (sends.at[b], kv_recv.at[b], to, tp)
            self.block = b

        def start(self):
            for blocks in (kall, vall):
                here = blocks.at[self.block]
                remote(here, here, *self.at).start()

        def wait_send(self):
            both = kall.at[pl.ds(0, 2)]
            remote(both, both, *self.at).wait_send()

        def wait_recv(self):
            both = kall.at[pl.ds(0, 2)]
            remote(both, both, *self.at).wait_recv()

    def next_copy(b):
        return KeyCopies(b, kv_next, sp + 2)

    def kv_sib_copy(b):
        return KeyCopies(b, kv_sib, sib)

    with SC('barrier_wait'):
        pl.semaphore_wait(barrier, n - 1 + tps - 1)

    @pl.when(z < zs - 1)
    def _():
        next_copy(sp).start()

    @pl.when(c == 0)
    def _():
        kv_sib_copy(sp).start()

    wd_start(1)

    depth = lax.broadcasted_iota(jnp.int32, (head_width, toks), 0)
    scale = half ** (-0.5)
    inputs[2].wait()
    split(2, store_rows)
    for h in range(heads):
        columns = turned(h) * scale
        qs[h, :, 0:toks] = jnp.where(depth < half, columns, 0.0).astype(BF16)
        qs[h, :, toks:] = jnp.where(depth >= half, columns, 0.0).astype(BF16)
    highs[...] = jnp.full_like(highs, -1e30)
    totals[...] = jnp.zeros_like(totals)
    acc[...] = jnp.zeros_like(acc)
    rows = lax.broadcasted_iota(jnp.int32, (toks, toks), 0)
    cols = lax.broadcasted_iota(jnp.int32, (toks, toks), 1)
    eye = rows == cols

    def process(b, masked):
        for h in range(heads):
            scores = mixed_dot(kall[b, head_rows(h), :], qs[h], ((1,), (0,)))
            if masked:
                scores = jnp.where(jnp.concatenate([rows <= cols] * 2, axis=1), scores, -1e30)
            old = highs[h]
            high = jnp.maximum(old, jnp.max(scores, axis=0, keepdims=True))
            shrink = jnp.exp(old - high)
            weights = jnp.exp(scores - high)
            totals[h] = shrink * totals[h] + jnp.sum(weights, axis=0, keepdims=True)
            blended = mixed_dot(
                vall[b, h * head_width : (h + 1) * head_width, :], weights.astype(BF16),
                ((1,), (0,)),
            )
            acc[h] = shrink * acc[h] + blended
            highs[h] = high

    with SC('proc_own'):
        process(sp, True)

    for load in small:
        load.wait()
    first = route_ref[0:1, :]
    lead = lax.broadcasted_iota(jnp.int32, (8, toks), 0)
    member = jnp.logical_and(
        first >= lead * per_group, first < (lead + 1) * per_group
    ).astype(F32)
    earlier = mixed_dot(member.astype(BF16), (rows < cols).astype(BF16), ((1,), (0,)))
    slot = jnp.sum(member * (earlier + lead.astype(F32) * cap), axis=0, keepdims=True)
    slot_col = jnp.sum(jnp.where(eye, slot, 0.0), axis=1, keepdims=True)
    slots = GROUPS * cap
    sel[...] = (
        lax.broadcasted_iota(jnp.int32, (slots, toks), 0) == slot.astype(jnp.int32)
    ).astype(BF16)
    selt[...] = (
        lax.broadcasted_iota(jnp.int32, (toks, slots), 1) == slot_col.astype(jnp.int32)
    ).astype(BF16)
    names = lax.broadcasted_iota(jnp.int32, (experts, toks), 0)
    by_expert = jnp.zeros((experts, toks), F32)
    for k in range(route_ref.shape[0]):
        by_expert = by_expert + jnp.where(
            names == route_ref[k : k + 1, :], rw_ref[k : k + 1, :], 0.0
        )
    by_slot = exact_pick(by_expert, selt[...])
    table = by_slot[:, 0:cap]
    for g in range(1, GROUPS):
        table = table + by_slot[:, g * cap : (g + 1) * cap]
    meta[sp, 0:experts, :] = table

    @pl.when(c == 1)
    def _():
        kv_sib_copy(2 * z).wait_recv()
        process(2 * z, False)

    def give_credits(j):
        def credit(which, plane):
            pl.semaphore_signal(
                free_sem.at[which], inc=1, device_id={"sp": 2 * plane + c, "tp": tp},
                device_id_type=MESH,
            )

        @pl.when(jnp.logical_and(j == z, z == zs - 2))
        def _():
            credit(0, 0)

        @pl.when(jnp.logical_and(j == z, z == zs - 1))
        def _():
            credit(1, 0)
            credit(1, 1)

    def visit(j, carry):
        b = 2 * (z - j) + c
        other = 2 * (z - j) + 1 - c
        with SC('wait_b'):
            kv_sib_copy(b).wait_recv()

        @pl.when(z < zs - 1)
        def _():
            next_copy(b).start()

        kv_sib_copy(b).start()
        give_credits(j)
        with SC('proc_b'):
            process(b, False)
        with SC('wait_o'):
            kv_sib_copy(other).wait_recv()
        with SC('proc_o'):
            process(other, False)
        return carry

    lax.fori_loop(1, z + 1, visit, 0)

    for h in range(heads):
        blend = acc[h] * (1.0 / totals[h])
        mix = blend[:, :toks] - lam_ref[:, h : h + 1] * blend[:, toks:]
        mix = mix * lax.rsqrt(jnp.mean(mix * mix, axis=0, keepdims=True) + norm_eps)
        att[:, h * head_width : (h + 1) * head_width] = (mix.T * gain_ref[...]).astype(BF16)
    inputs[3].wait()

    def projected(to):
        return jnp.dot(
            att[...], owv[:, pl.ds(pl.multiple_of(to * piece, piece), piece)],
            preferred_element_type=F32,
        )

    half_toks = toks // 2
    part_halves = (slice(0, half_toks), slice(half_toks, toks))

    def rs_copy(i):
        to, source, target = [
            (beside, part.at[across, part_halves[0]], ppass.at[0]),
            (above, part.at[across, part_halves[1]], ppass.at[1]),
            (beside, part.at[beside, part_halves[0]], rbuf.at[0, part_halves[0]]),
            (above, part.at[above, part_halves[1]], rbuf.at[1, part_halves[1]]),
            (above, part.at[above, part_halves[0]], rbuf.at[1, part_halves[0]]),
            (beside, part.at[beside, part_halves[1]], rbuf.at[0, part_halves[1]]),
        ][i]
        return remote(source, target, rs_send, rs_recv.at[min(i, 2)], sp, to)

    part[across] = projected(across).astype(BF16)
    rs_copy(0).start()
    rs_copy(1).start()
    for_beside = projected(beside)
    part[beside, part_halves[0]] = for_beside[part_halves[0]].astype(BF16)
    rs_copy(2).start()
    for_above = projected(above)
    part[above, part_halves[1]] = for_above[part_halves[1]].astype(BF16)
    rs_copy(3).start()
    mine = pl.ds(pl.multiple_of(tp * piece, piece), piece)
    inputs[4].wait()
    total = resv[:, mine].astype(F32) + projected(tp)
    with SC("rs_pass"):
        rs_copy(0).wait_recv()
    part[above, part_halves[0]] = (for_above[part_halves[0]] + ppass[0].astype(F32)).astype(BF16)
    rs_copy(4).start()
    with SC("rs_pass"):
        rs_copy(1).wait_recv()
    part[beside, part_halves[1]] = (for_beside[part_halves[1]] + ppass[1].astype(F32)).astype(BF16)
    rs_copy(5).start()
    wd_start(2)

    half_cap = cap // 2

    def spot(src, core, part):
        return xall.at[
            src,
            pl.ds(pl.multiple_of(core * cap, cap), cap),
            pl.ds(pl.multiple_of(part * piece, piece), piece),
        ]

    def half_spot(src, part, side):
        return xall.at[
            src,
            pl.ds(pl.multiple_of(c * cap + side * half_cap, half_cap), half_cap),
            pl.ds(pl.multiple_of(part * piece, piece), piece),
        ]

    def x_copy(s):
        group = (z + s) % zs
        return remote(
            xs.at[s], spot(z, c, tp), x_send, x_recv.at[z, 0], 2 * group + c, tp
        )

    def spot_wait(here, sem):
        remote(here, here, x_send, sem, sib, tp).wait_recv()

    def tp_copy(src, i):
        to, side = [(beside, 0), (above, 1), (beside, 1), (above, 0)][i]
        here = half_spot(src, tp, side)
        return remote(here, here, x_tp, x_recv.at[src, 1 + i], sp, to)

    def pass_copy(src, i):
        part, side, to = [(beside, 0, above), (above, 1, beside)][i]
        here = half_spot(src, part, side)
        return remote(here, here, x_tp, x_recv.at[src, 5], sp, to)

    def sib_copy(src, part):
        here = spot(src, c, part)
        return remote(here, here, x_sib, s_recv.at[src], sib, tp)

    def gather(src):
        @pl.when(src != z)
        def _():
            with SC("arrive"):
                spot_wait(spot(src, c, tp), x_recv.at[src, 0])

        for i in range(4):
            tp_copy(src, i).start()
        sib_copy(src, tp).start()

    def gather_pass(src):
        with SC("gpass"):
            spot_wait(half_spot(src, beside, 0), x_recv.at[src, 1])
        pass_copy(src, 0).start()
        with SC("gpass"):
            spot_wait(half_spot(src, above, 1), x_recv.at[src, 2])
        pass_copy(src, 1).start()

    def forward(src):
        with SC("compl_tp"):
            spot_wait(half_spot(src, beside, 1), x_recv.at[src, 3])
            sib_copy(src, beside).start()
            spot_wait(half_spot(src, above, 0), x_recv.at[src, 4])
            sib_copy(src, above).start()
            spot_wait(spot(src, c, across), x_recv.at[src, 5])
            sib_copy(src, across).start()

    def complete(src):
        with SC("compl_sib"):
            spot_wait(
                xall.at[src, pl.ds(pl.multiple_of((1 - c) * cap, cap), cap)], s_recv.at[src]
            )

    pl.when(z > 0)(lambda: gather(0))
    pl.when(z == zs - 2)(lambda: gather(1))

    with SC("rs_wait"):
        remote(rbuf, rbuf, rs_send, rs_recv.at[2], sp, beside).wait_recv()
    total = total + rbuf[0].astype(F32) + rbuf[1].astype(F32)
    stream_ref[...] = total
    normed_ref[...] = (total * fg_ref[:, mine]).astype(BF16)
    squares = jnp.sum(total * total, axis=1, keepdims=True)
    as_row = jnp.sum(jnp.where(eye, squares, 0.0), axis=0, keepdims=True)
    sq_send[...] = jnp.broadcast_to(as_row, sq_send.shape)

    def sq_copy(d):
        return remote(
            sq_send, sq_recv.at[d], sq_ss, sq_rs, sp, (tp + d) % tps
        )

    for d in range(1, tps):
        sq_copy(d).start()

    def m_copy(d):
        return remote(meta.at[sp], meta.at[sp], m_send, m_recv.at[sp], (sp + d) % n, tp)

    def m_wait(src):
        @pl.when(src != sp)
        def _():
            remote(meta.at[src], meta.at[src], m_send, m_recv.at[src], sib, tp).wait_recv()

    for s in list(range(1, zs)) + [0]:
        group = (z + s) % zs
        picked = jnp.dot(
            sel[pl.ds(pl.multiple_of(group * cap, cap), cap), :], normed_ref[...],
            preferred_element_type=F32,
        ).astype(BF16)
        if s:
            xs[s] = picked
            pl.when(z >= (zs - s if s >= zs - 2 else 0))(lambda: x_copy(s).start())
        else:
            spot(z, c, tp)[...] = picked

    @pl.when(z < zs - 1)
    def _():
        gather(z)

    wd_start(3)

    def row_factors():
        with SC("sq_wait"):
            squares_in = sq_recv.at[pl.ds(1, tps - 1)]
            remote(squares_in, squares_in, sq_ss, sq_rs, sp, beside).wait_recv()
        sums = sq_send[0:1, :]
        for d in range(1, tps):
            sums = sums + sq_recv[d, 0:1, :]
        inverse = lax.rsqrt(sums * (1.0 / (piece * tps)) + norm_eps)
        by_slot = exact_pick(jnp.broadcast_to(inverse, (8, toks)), selt[...])
        for g in range(GROUPS):
            meta[sp, experts + g : experts + g + 1, :] = by_slot[0:1, g * cap : (g + 1) * cap]
        for d in range(1, n):
            m_copy(d).start()

    def late_rows(s, which):
        with SC("credit"):
            pl.semaphore_wait(free_sem.at[which], 1)
        x_copy(s).start()

    pl.when(z < zs - 2)(row_factors)
    gather_pass(0)

    @pl.when(z == zs - 2)
    def _():
        gather_pass(1)
        gather_pass(2)

    pl.when(z == zs - 1)(lambda: gather(1))
    wd_start(4)
    pl.when(z == zs - 2)(row_factors)
    pl.when(z == 1)(lambda: late_rows(zs - 2, 1))

    @pl.when(z == 0)
    def _():
        late_rows(zs - 2, 0)
        gather(1)
        late_rows(zs - 1, 1)

    def late_sources():
        gather(zs - 2)
        pl.when(z == 0)(lambda: gather_pass(1))
        wd_start(5)
        forward(1)
        gather_pass(zs - 2)
        wd_start(6)

    def near_copy(src, part):
        return remote(
            away.at[src, part], near.at[src, part], n_send,
            n_recv.at[src, jnp.where(part == across, 0, 1)], sib, tp,
        )

    def near_wait(src, first):
        here = near.at[src, pl.ds(0, 1 if first else tps - 1)]
        remote(here, here, n_send, n_recv.at[src, 0 if first else 1], sib, tp).wait_recv()

    tile = 256
    small_eye = lax.broadcasted_iota(jnp.int32, (cap, cap), 0) == lax.broadcasted_iota(
        jnp.int32, (cap, cap), 1
    )
    which = lax.broadcasted_iota(jnp.int32, meta.shape[1:], 0)

    def meta_col(src, core, line):
        row = jnp.sum(jnp.where(which == line, meta[2 * src + core], 0.0), axis=0, keepdims=True)
        return jnp.sum(jnp.where(small_eye, row, 0.0), axis=1, keepdims=True)

    keep_rows = pl.ds(pl.multiple_of(c * cap, cap), cap)
    away_rows = pl.ds(pl.multiple_of((1 - c) * cap, cap), cap)

    def ffn_one(src, between):
        @pl.when(src == 0)
        def _():
            for load in loads:
                load.wait()

        with SC("m_wait"):
            m_wait(2 * src)
            m_wait(2 * src + 1)
        factor = jnp.concatenate(
            [meta_col(src, c, experts + z), meta_col(src, 1 - c, experts + z)], axis=0
        )

        def one(i, carry):
            pl.when(i == wg.shape[1] // tile // 2)(between)
            at = pl.ds(pl.multiple_of(i * tile, tile), tile)
            x = jnp.concatenate([xall[src, keep_rows], xall[src, away_rows]], axis=0)
            gate = jnp.dot(x, wg[:, at], preferred_element_type=F32) * factor
            up = jnp.dot(x, wu[:, at], preferred_element_type=F32) * factor
            hid[src, :, at] = (gate / (1.0 + jnp.exp(-gate)) * up).astype(BF16)
            return carry

        with SC("ffn_one"):
            lax.fori_loop(0, wg.shape[1] // tile, one, 0)

    def ffn_two(src, first):
        @pl.when(first)
        def _():
            with SC("down_wait"):
                others = wdv.at[pl.ds(0, tps - 1)]
                remote(others, others, wd_send, wd_recv, sp, beside).wait()

        row_weight = jnp.concatenate(
            [meta_col(src, c, sp), meta_col(src, 1 - c, sp)], axis=0
        )

        def two(j, carry):
            to = tp ^ (tps - 1 - j)
            result = jnp.dot(hid[src], wdv[to], preferred_element_type=F32) * row_weight
            away[src, to] = result[cap:].astype(BF16)
            near_copy(src, to).start()
            keep[src, to] = result[:cap]
            return carry

        with SC("ffn_two"):
            lax.fori_loop(0, tps, two, 0)

    cap_halves = (slice(0, half_cap), slice(half_cap, cap))

    def r_copy(src, i):
        to, source, target = [
            (beside, rsend.at[src, across, cap_halves[0]], rpass.at[src, 0]),
            (above, rsend.at[src, across, cap_halves[1]], rpass.at[src, 1]),
            (beside, rsend.at[src, beside, cap_halves[0]], rrecv.at[src, 0, cap_halves[0]]),
            (above, rsend.at[src, above, cap_halves[1]], rrecv.at[src, 1, cap_halves[1]]),
            (above, rsend.at[src, above, cap_halves[0]], rrecv.at[src, 1, cap_halves[0]]),
            (beside, rsend.at[src, beside, cap_halves[1]], rrecv.at[src, 0, cap_halves[1]]),
        ][i]
        return remote(source, target, r_send, r_recv.at[src, min(i, 2)], sp, to)

    def both(src, to, at):
        return keep[src, to, at, :] + near[src, to, at, :].astype(F32)

    def spread(src):
        with SC("near_wait"):
            near_wait(src, True)
        rsend[src, across] = both(src, across, slice(0, cap)).astype(BF16)
        r_copy(src, 0).start()
        r_copy(src, 1).start()
        near_wait(src, False)
        rsend[src, above, cap_halves[1]] = both(src, above, cap_halves[1]).astype(BF16)
        r_copy(src, 3).start()
        rsend[src, beside, cap_halves[0]] = both(src, beside, cap_halves[0]).astype(BF16)
        r_copy(src, 2).start()

    def spread_pass(src):
        with SC("spass"):
            r_copy(src, 0).wait_recv()
        rsend[src, above, cap_halves[0]] = (
            both(src, above, cap_halves[0]) + rpass[src, 0].astype(F32)
        ).astype(BF16)
        r_copy(src, 4).start()
        with SC("spass"):
            r_copy(src, 1).wait_recv()
        rsend[src, beside, cap_halves[1]] = (
            both(src, beside, cap_halves[1]) + rpass[src, 1].astype(F32)
        ).astype(BF16)
        r_copy(src, 5).start()

    def b_copy(src):
        return remote(
            back.at[src], ret.at[z], b_send, b_recv, 2 * src + c, tp
        )

    def finish(src):
        with SC("r_wait"):
            here = rrecv.at[src]
            remote(here, here, r_send, r_recv.at[src, 2], sp, beside).wait_recv()
        total = both(src, tp, slice(0, cap))
        total = total + rrecv[src, 0].astype(F32) + rrecv[src, 1].astype(F32)

        @pl.when(src == z)
        def _():
            ret[z] = total.astype(BF16)

        @pl.when(src != z)
        def _():
            back[src] = total.astype(BF16)
            b_copy(src).start()

    last = zs - 1

    at_last = z == last

    early = z < last

    def when_both(one, two):
        return pl.when(jnp.logical_and(one, two))

    third = z == last - 1
    first_two = z < last - 1
    lead = jnp.where(first_two, last - 1, 0)
    after = jnp.where(z == 1, 0, 1)

    def up_step(s):
        def between():
            when_both(third, s == 0)(lambda: forward(1))
            when_both(z == 1, s == 0)(lambda: gather_pass(1))
            when_both(early, s == 1)(lambda: forward(2))
            when_both(early, s == last - 1)(lambda: gather(last))
            when_both(early, s == last)(lambda: finish(lead))
            when_both(early, s == last)(lambda: spread_pass(after))
            when_both(at_last, s < last)(lambda: gather_pass(s + 1))
            when_both(at_last, s + 2 <= last)(lambda: gather(s + 2))

        pl.when(s == 0)(lambda: forward(0))
        when_both(at_last, s == 0)(row_factors)
        when_both(first_two, s == 1)(late_sources)
        complete(s)
        ffn_one(s, between)
        when_both(at_last, s == last)(lambda: spread_pass(last - 1))

    def down_step(s):
        ffn_two(s, s == jnp.where(early, lead, 0))
        when_both(at_last, s < last)(lambda: forward(s + 1))
        when_both(early, s == lead)(lambda: gather_pass(last))
        when_both(early, s == after)(lambda: spread_pass(lead))
        when_both(early, s == z)(lambda: spread_pass(last))
        when_both(at_last, jnp.logical_and(s >= 1, s < last))(lambda: spread_pass(s - 1))
        spread(s)
        when_both(early, s == after)(lambda: forward(last))
        when_both(early, s == last)(lambda: finish(after))
        when_both(at_last, s == last - 1)(lambda: finish(0))

        @pl.when(jnp.logical_and(at_last, s == last))
        def _():
            finish(1)
            finish(2)

    def step(k, carry):
        turn = k
        for at, value in enumerate(
            (0, 2, 4, 2 * lead + 1, 2 * after + 1, 2 * last, 2 * last + 1, 2 * z + 1)
        ):
            turn = jnp.where(jnp.logical_and(early, k == at), value, turn)
        pl.when(turn % 2 == 0)(lambda: up_step(turn // 2))
        pl.when(turn % 2 == 1)(lambda: down_step(turn // 2))
        return carry

    lax.fori_loop(0, 2 * zs, step, 0)
    pl.when(at_last)(lambda: spread_pass(last))
    finish(last)

    @pl.when(early)
    def _():
        spread_pass(z)
        finish(z)

    with SC("b_wait"):
        returns = ret.at[pl.ds(0, zs - 1)]
        remote(returns, returns, b_send, b_recv, sib, tp).wait_recv()
    rows = ret[...].reshape(zs * cap, piece)
    layer = stream_ref[...] + jnp.dot(selt[...], rows, preferred_element_type=F32)
    outv[:, mine] = layer.astype(BF16)

    def out_spot(part, side):
        return outv.at[part_halves[side], pl.ds(pl.multiple_of(part * piece, piece), piece)]

    def o_copy(i):
        part, side, to = [
            (tp, 0, beside), (tp, 1, above), (tp, 1, beside), (tp, 0, above),
            (beside, 0, above), (above, 1, beside),
        ][i]
        here = out_spot(part, side)
        return remote(here, here, o_send, o_recv.at[min(i, 4)], sp, to)

    def o_wait(part, i, side=None):
        at = pl.ds(pl.multiple_of(part * piece, piece), piece)
        here = outv.at[:, at] if side is None else out_spot(part, side)
        remote(here, here, o_send, o_recv.at[i], sib, tp).wait_recv()

    for i in range(4):
        o_copy(i).start()
    with SC("o_pass"):
        o_wait(beside, 0, 0)
    o_copy(4).start()
    with SC("o_pass"):
        o_wait(above, 1, 1)
    o_copy(5).start()

    def sent(here, sem):
        remote(here, here, sem, kv_recv.at[0], sib, tp).wait_send()

    sent(sq_recv.at[pl.ds(1, tps - 1)], sq_ss)
    sent(part.at[pl.ds(0, 3)], rs_send)
    sent(meta.at[pl.ds(0, n - 1)], m_send)
    sent(xs.at[pl.ds(1, zs - 1)], x_send)
    sent(back.at[pl.ds(0, zs - 1)], b_send)
    sent(away, n_send)
    sent(away, x_sib)
    sent(away.at[pl.ds(0, zs - 1)], x_tp)
    sent(away.at[pl.ds(0, zs - 1)], r_send)

    @pl.when(z < zs - 1)
    def _():
        next_copy(sp).wait_send()

    @pl.when(c == 0)
    def _():
        kv_sib_copy(sp).wait_send()

    def drain(j, carry):
        b = 2 * (z - j) + c

        @pl.when(z < zs - 1)
        def _():
            next_copy(b).wait_send()

        kv_sib_copy(b).wait_send()
        return carry

    lax.fori_loop(1, z + 1, drain, 0)
    with SC("o_wait"):
        o_wait(beside, 2, 1)
        o_wait(above, 3, 0)
        o_wait(across, 4)
    with SC("o_send"):
        sent(part.at[pl.ds(0, 3)], o_send)


def paired_shards(
    residual, queries, key_vectors, value_rows, head_lambda, head_gain, out_weight, ffn_gain,
    expert_gate, expert_up, expert_down, routing, route_weight,
):
    n = lax.axis_size("sp")
    tps = lax.axis_size("tp")
    toks, heads, head_width = queries.shape
    width = heads * head_width
    model = residual.shape[1]
    piece = model // tps
    experts = n
    per_group = experts // GROUPS
    cap = toks // per_group
    down = expert_down[0]
    wd_rows = down.shape[0] // tps
    vmem = pl.BlockSpec(memory_space=pltpu.VMEM)
    hbm = pl.BlockSpec(memory_space=pltpu.HBM)
    dma = pltpu.SemaphoreType.DMA
    zs = n // 2
    def stay(x):
        return pltpu.with_memory_space_constraint(x, pltpu.HBM)

    return pl.pallas_call(
        functools.partial(layer_kernel, n, tps, cap, heads, head_width),
        out_shape=jax.ShapeDtypeStruct((toks, model), BF16),
        in_specs=[hbm] * 13,
        out_specs=vmem,
        scratch_shapes=[
            pltpu.VMEM(routing.shape[::-1], jnp.int32),
            pltpu.VMEM(route_weight.shape[::-1], F32),
            pltpu.VMEM((1, heads), F32),
            pltpu.VMEM((1, head_width), F32),
            pltpu.VMEM((1, model), F32),
            pltpu.VMEM((3, toks * heads, head_width), BF16),
            pltpu.VMEM((toks, model), BF16),
            pltpu.VMEM((width, model), BF16),
            pltpu.VMEM((GROUPS * cap, toks), BF16),
            pltpu.VMEM((toks, GROUPS * cap), BF16),
            pltpu.VMEM((toks, piece), F32),
            pltpu.VMEM((toks, piece), BF16),
            pltpu.VMEM((n, experts + 8, cap), F32),
            pltpu.VMEM((zs, cap, piece), BF16),
            pltpu.VMEM((zs, 2 * cap, model), BF16),
            pltpu.VMEM(expert_gate.shape[1:], BF16),
            pltpu.VMEM(expert_up.shape[1:], BF16),
            pltpu.VMEM((tps, wd_rows, piece), BF16),
            pltpu.VMEM((zs, 2 * cap, expert_gate.shape[2]), BF16),
            pltpu.VMEM((zs, tps, cap, piece), F32),
            pltpu.VMEM((zs, tps, cap, piece), BF16),
            pltpu.VMEM((zs, tps, cap, piece), BF16),
            pltpu.VMEM((zs, tps, cap, piece), BF16),
            pltpu.VMEM((zs, 2, cap, piece), BF16),
            pltpu.VMEM((zs, 2, cap // 2, piece), BF16),
            pltpu.VMEM((zs, cap, piece), BF16),
            pltpu.VMEM((zs, cap, piece), BF16),
            pltpu.VMEM((n, heads * toks, head_width), BF16),
            pltpu.VMEM((n, width, toks), BF16),
            pltpu.VMEM((heads * toks, head_width), BF16),
            pltpu.VMEM((heads, head_width, 2 * toks), BF16),
            pltpu.VMEM((heads, 1, 2 * toks), F32),
            pltpu.VMEM((heads, 1, 2 * toks), F32),
            pltpu.VMEM((heads, head_width, 2 * toks), F32),
            pltpu.VMEM((toks, width), BF16),
            pltpu.VMEM((tps, toks, piece), BF16),
            pltpu.VMEM((2, toks, piece), BF16),
            pltpu.VMEM((2, toks // 2, piece), BF16),
            pltpu.VMEM((8, toks), F32),
            pltpu.VMEM((tps, 8, toks), F32),
            dma((10,)), dma((3,)),
            dma, dma, dma, dma((zs, 6)), dma((zs,)),
            dma, dma((zs, 2)), dma, dma((zs, 3)),
            dma, dma, dma, dma((5,)),
            dma((n,)), dma((n,)), dma((n,)),
            dma, dma, dma, dma((n,)),
            dma, dma((3,)), dma, dma, pltpu.SemaphoreType.REGULAR((2,)),
        ],
        compiler_params=pltpu.CompilerParams(collective_id=0, has_side_effects=True, vmem_limit_bytes=49545216),
        name="layer",
    )(
        stay(queries.reshape(toks * heads, head_width)), stay(key_vectors.reshape(toks * heads, head_width)),
        stay(value_rows.reshape(toks * heads, head_width)), stay(routing.T), stay(route_weight.T), stay(down),
        stay(head_lambda.reshape(1, -1)), stay(head_gain.reshape(1, -1)), stay(out_weight), stay(residual), stay(ffn_gain.reshape(1, -1)),
        stay(expert_gate), stay(expert_up),
    )


def solution(mesh):
    in_specs = (
        P("sp", None),
        P("sp", "tp", None),
        P("sp", "tp", None),
        P("sp", "tp", None),
        P("tp"),
        P(),
        P("tp", None),
        P(),
        P("sp", None, "tp"),
        P("sp", None, "tp"),
        P("sp", None, "tp"),
        P("sp", None),
        P("sp", None),
    )
    out_specs = P("sp", None)
    paired = mesh.shape["sp"] == 2 * GROUPS and mesh.shape["tp"] == 4
    return jax.shard_map(paired_shards if paired else shards, mesh=mesh, in_specs=in_specs, out_specs=out_specs, check_vma=False)
```

```python
import functools
import math

import jax
import jax.numpy as jnp
from jax import lax
from jax.experimental import pallas as pl
from jax.experimental.pallas import tpu as pltpu
from jax.sharding import PartitionSpec as P

GROUPS = 4
SC = jax.named_scope


norm_eps = 1e-06


def online_update(running, query_part, key_part, value_part, query_pos, key_pos, score_scale):
    highest, totals, accum = running
    scores = (
        jnp.einsum("qhd,khd->hqk", query_part, key_part, preferred_element_type=jnp.float32)
        * score_scale
    )
    scores = jnp.where(key_pos[None, None, :] <= query_pos[None, :, None], scores, -jnp.inf)
    new_high = jnp.maximum(highest, jnp.max(scores, axis=-1))
    shrink = jnp.exp(highest - new_high)
    weights = jnp.exp(scores - new_high[:, :, None])
    totals = shrink * totals + jnp.sum(weights, axis=-1)
    blended = jnp.einsum(
        "hqk,khe->qhe", weights.astype(jnp.bfloat16), value_part, preferred_element_type=jnp.float32
    )
    accum = jnp.transpose(shrink)[:, :, None] * accum + blended
    return (new_high, totals, accum)


def shards(
    residual,
    queries,
    key_vectors,
    value_rows,
    head_lambda,
    head_gain,
    out_weight,
    ffn_gain,
    expert_gate,
    expert_up,
    expert_down,
    routing,
    route_weight,
):
    tok_count = queries.shape[0]
    local_heads = queries.shape[1]
    half_width = queries.shape[2] // 2
    value_width = value_rows.shape[2]
    score_scale = half_width ** (-0.5)
    query_pos = lax.axis_index("sp") * tok_count + jnp.arange(tok_count, dtype=jnp.int32)
    last_query = query_pos[-1]
    first_half = queries[:, :, :half_width]
    second_half = queries[:, :, half_width:]
    start_high = jnp.full((local_heads, tok_count), -1e30, jnp.float32)
    start_total = jnp.zeros((local_heads, tok_count), jnp.float32)
    start_accum = jnp.zeros((tok_count, local_heads, value_width), jnp.float32)
    empty_state = (start_high, start_total, start_accum)
    running = (empty_state, empty_state)
    key_piece = lax.all_gather(key_vectors, "sp", axis=0, tiled=True)
    value_piece = lax.all_gather(value_rows, "sp", axis=0, tiled=True)
    piece_len = key_piece.shape[0]
    block_len = math.gcd(piece_len, 512)
    block_count = piece_len // block_len
    key_blocks = key_piece.reshape(block_count, block_len, local_heads, 2 * half_width)
    value_blocks = value_piece.reshape(block_count, block_len, local_heads, value_width)

    def visit(current, stacked):
        block_index, key_block, value_block = stacked
        block_first = block_index * block_len
        key_pos = block_first + jnp.arange(block_len, dtype=jnp.int32)

        def compute(inside):
            first_state = online_update(
                inside[0],
                first_half,
                key_block[:, :, :half_width],
                value_block,
                query_pos,
                key_pos,
                score_scale,
            )
            second_state = online_update(
                inside[1],
                second_half,
                key_block[:, :, half_width:],
                value_block,
                query_pos,
                key_pos,
                score_scale,
            )
            return (first_state, second_state)

        return (lax.cond(block_first <= last_query, compute, lambda inside: inside, current), None)

    running, _ = lax.scan(
        visit, running, (jnp.arange(block_count, dtype=jnp.int32), key_blocks, value_blocks)
    )
    first_state, second_state = running
    first_out = first_state[2] / jnp.transpose(first_state[1])[:, :, None]
    second_out = second_state[2] / jnp.transpose(second_state[1])[:, :, None]
    combined = first_out - head_lambda[None, :, None] * second_out
    normed_heads = (
        combined
        * lax.rsqrt(jnp.mean(combined * combined, axis=-1, keepdims=True) + norm_eps)
        * head_gain
    )
    attended = normed_heads.astype(jnp.bfloat16).reshape(tok_count, local_heads * value_width)
    partial_proj = jnp.dot(attended, out_weight, preferred_element_type=jnp.float32)
    projected = lax.psum(partial_proj.astype(jnp.bfloat16), "tp").astype(jnp.float32)
    stream = residual.astype(jnp.float32) + projected
    block_normed = (
        stream * lax.rsqrt(jnp.mean(stream * stream, axis=-1, keepdims=True) + norm_eps) * ffn_gain
    ).astype(jnp.bfloat16)
    expert_count = lax.axis_size("sp")
    tp_count = lax.axis_size("tp")
    per_group = expert_count // GROUPS
    capacity = tok_count // per_group
    top_count = routing.shape[1]
    model_width = block_normed.shape[1]
    flat_routes = routing.reshape(-1)
    route_count = flat_routes.shape[0]
    onehot = (flat_routes[:, None] == jnp.arange(expert_count, dtype=jnp.int32)[None, :]).astype(
        jnp.int32
    )
    earlier = jnp.cumsum(onehot, axis=0) - onehot
    position = jnp.sum(earlier * onehot, axis=1)
    slot_index = flat_routes * capacity + position
    slot_token = (
        jnp.full((expert_count * capacity,), tok_count, jnp.int32)
        .at[slot_index]
        .set(jnp.arange(route_count, dtype=jnp.int32) // top_count)
    )
    slot_table = slot_token.reshape(expert_count, capacity)
    slice_width = model_width // tp_count
    own_columns = lax.dynamic_slice_in_dim(
        block_normed, lax.axis_index("tp") * slice_width, slice_width, 1
    )
    outgoing = jnp.take(own_columns, slot_table, axis=0, mode="fill", fill_value=0)
    landed = lax.all_to_all(outgoing, "sp", split_axis=0, concat_axis=0, tiled=True)
    arrived = lax.all_gather(landed, "tp", axis=2, tiled=True)
    expert_rows = arrived.reshape(-1, model_width)
    gate_part = jnp.dot(expert_rows, expert_gate[0], preferred_element_type=jnp.float32)
    up_part = jnp.dot(expert_rows, expert_up[0], preferred_element_type=jnp.float32)
    inner_act = (jax.nn.silu(gate_part) * up_part).astype(jnp.bfloat16)
    down_width = expert_down.shape[2]
    weight_rows = expert_down[0]
    expert_sum = jnp.dot(
        lax.all_gather(inner_act, "tp", axis=1, tiled=True),
        weight_rows,
        preferred_element_type=jnp.float32,
    )
    expert_out = expert_sum.astype(jnp.bfloat16).reshape(expert_count, capacity, down_width)
    returned = lax.all_to_all(expert_out, "sp", split_axis=0, concat_axis=0, tiled=True)
    per_route = returned.reshape(expert_count * capacity, down_width)[slot_index]
    weighted = per_route.astype(jnp.float32) * route_weight.reshape(-1)[:, None]
    token_sum = jnp.sum(weighted.reshape(tok_count, top_count, down_width), axis=1)
    moe_rows = lax.all_gather(token_sum.astype(jnp.bfloat16), "tp", axis=1, tiled=True).astype(
        token_sum.dtype
    )
    return (stream + moe_rows).astype(jnp.bfloat16)


MESH = pl.DeviceIdType.MESH
F32 = jnp.float32
BF16 = jnp.bfloat16


def remote(src, dst, send_sem, recv_sem, sp, tp):
    return pltpu.make_async_remote_copy(
        src_ref=src,
        dst_ref=dst,
        send_sem=send_sem,
        recv_sem=recv_sem,
        device_id={"sp": sp, "tp": tp},
        device_id_type=MESH,
    )


def mixed_dot(left, right, contract):
    return lax.dot_general(left, right, (contract, ((), ())), preferred_element_type=F32)


def dispersed(value):
    high = value.astype(BF16)
    rest = value - high.astype(F32)
    middle = rest.astype(BF16)
    low = (rest - middle.astype(F32)).astype(BF16)
    return jnp.concatenate([high, middle, low], axis=0)


def exact_pick(value, picker):
    count = value.shape[0]
    parts = mixed_dot(dispersed(value), picker, ((1,), (0,)))
    return parts[:count] + parts[count : 2 * count] + parts[2 * count :]


def layer_kernel(
    n, tps, cap, heads, head_width,
    q_ref, k_ref, v_ref, route_in, rw_in, wd_ref, lam_in, gain_in, ow_ref, res_ref, fg_in,
    gate_ref, up_ref,
    outv,
    route_ref, rw_ref, lam_ref, gain_ref, fg_ref, raw, resv, owv, sel, selt, stream_ref, normed_ref, meta,
    xs, xall, wg, wu, wdv, hid, keep, away, near, rsend, rrecv, rpass, back, ret,
    kall, vall, rowm, qs, highs, totals, acc, att, part, rbuf, ppass, sq_send, sq_recv,
    in_sem, w_sem, x_send, x_tp, x_sib, x_recv, s_recv, n_send, n_recv, r_send, r_recv,
    b_send, b_recv, o_send, o_recv,
    kv_next, kv_sib, kv_recv, wd_send, wd_recv, m_send, m_recv,
    rs_send, rs_recv, sq_ss, sq_rs, free_sem,
):
    sp = lax.axis_index("sp")
    tp = lax.axis_index("tp")
    z, c = sp // 2, sp % 2
    zs = n // 2
    sib = 2 * z + 1 - c
    toks = resv.shape[0]
    width = heads * head_width
    half = head_width // 2
    piece = normed_ref.shape[1]
    wd_rows = wdv.shape[1]
    experts = n
    per_group = experts // GROUPS
    beside, above, across = tp ^ 1, tp ^ 2, tp ^ 3

    barrier = pltpu.get_barrier_semaphore()
    for d in range(1, n):
        pl.semaphore_signal(
            barrier, inc=1, device_id={"sp": (sp + d) % n, "tp": tp}, device_id_type=MESH
        )
    for d in range(1, tps):
        pl.semaphore_signal(
            barrier, inc=1, device_id={"sp": sp, "tp": (tp + d) % tps}, device_id_type=MESH
        )
    inputs = [
        pltpu.make_async_copy(k_ref, raw.at[0], in_sem.at[0]),
        pltpu.make_async_copy(v_ref, raw.at[1], in_sem.at[1]),
        pltpu.make_async_copy(q_ref, raw.at[2], in_sem.at[2]),
        pltpu.make_async_copy(ow_ref, owv, in_sem.at[3]),
        pltpu.make_async_copy(res_ref, resv, in_sem.at[4]),
    ]
    small = [
        pltpu.make_async_copy(given, kept, in_sem.at[5 + i])
        for i, (given, kept) in enumerate(
            (
                (route_in, route_ref), (rw_in, rw_ref), (lam_in, lam_ref), (gain_in, gain_ref),
                (fg_in, fg_ref),
            )
        )
    ]
    loads = [
        pltpu.make_async_copy(gate_ref.at[0], wg, w_sem.at[0]),
        pltpu.make_async_copy(up_ref.at[0], wu, w_sem.at[1]),
        pltpu.make_async_copy(
            wd_ref.at[pl.ds(pl.multiple_of(tp * wd_rows, wd_rows), wd_rows), :],
            wdv.at[tp], w_sem.at[2],
        ),
    ]
    for load in inputs + small + loads:
        load.start()

    run = toks // heads
    spot_row = lax.broadcasted_iota(jnp.int32, (run, toks), 0)
    spot_col = lax.broadcasted_iota(jnp.int32, (run, toks), 1)
    order = jnp.concatenate(
        [(spot_col == spot_row * heads + h).astype(BF16) for h in range(heads)], axis=0
    )

    def split(which, store):
        for i in range(heads):
            rows = jnp.dot(
                order, raw[which, i * toks : (i + 1) * toks, :], preferred_element_type=F32
            )
            for h in range(heads):
                store(i, h, rows[h * run : (h + 1) * run, :])

    def head_rows(h, i=0, count=toks):
        return slice(h * toks + i * run, h * toks + i * run + count)

    def store_keys(i, h, rows):
        kall[sp, head_rows(h, i, run), :] = rows.astype(BF16)

    def store_rows(i, h, rows):
        rowm[head_rows(h, i, run), :] = rows.astype(BF16)

    unit = (
        lax.broadcasted_iota(jnp.int32, (head_width, head_width), 0)
        == lax.broadcasted_iota(jnp.int32, (head_width, head_width), 1)
    ).astype(BF16)

    def turned(h):
        return mixed_dot(unit, rowm[head_rows(h), :], ((1,), (1,)))

    inputs[0].wait()
    split(0, store_keys)
    inputs[1].wait()
    split(1, store_rows)
    for h in range(heads):
        vall[sp, h * head_width : (h + 1) * head_width, :] = turned(h).astype(BF16)

    chunks = 8
    wd_run = wd_rows // chunks

    def wd_copy(k, d):
        to = tp ^ d
        return remote(
            wd_ref.at[pl.ds(pl.multiple_of(to * wd_rows + k * wd_run, wd_run), wd_run), :],
            wdv.at[tp, pl.ds(pl.multiple_of(k * wd_run, wd_run), wd_run)],
            wd_send, wd_recv, sp, to,
        )

    def by_plane(values):
        chosen = values[-1]
        for plane, value in enumerate(values[:-1]):
            chosen = jnp.where(z == plane, value, chosen)
        return chosen

    wd_points = [
        (0, 0, 0, 0), (1, 3, 5, 7), (2, 4, 6, 7), (3, 4, 6, 7), (6, 6, 8, 8), (7, 7, 8, 8), (8, 8, 8, 8)
    ]

    def wd_start(point):
        def start(k, carry):
            for d in (3, 1, 2):
                wd_copy(k, d).start()
            return carry

        lax.fori_loop(by_plane(wd_points[point - 1]), by_plane(wd_points[point]), start, 0)

    class KeyCopies:
        def __init__(self, b, sends, to):
            self.at = (sends.at[b // 2], kv_recv.at[b], to, tp)
            self.block = b

        def start(self):
            for blocks in (kall, vall):
                here = blocks.at[self.block]
                remote(here, here, *self.at).start()

        def wait_send(self):
            both = kall.at[pl.ds(0, 2)]
            remote(both, both, *self.at).wait_send()

        def wait_recv(self):
            both = kall.at[pl.ds(0, 2)]
            remote(both, both, *self.at).wait_recv()

    def next_copy(b):
        return KeyCopies(b, kv_next, sp + 2)

    def kv_sib_copy(b):
        return KeyCopies(b, kv_sib, sib)

    with SC('barrier_wait'):
        pl.semaphore_wait(barrier, n - 1 + tps - 1)

    @pl.when(z < zs - 1)
    def _():
        next_copy(sp).start()

    @pl.when(c == 0)
    def _():
        kv_sib_copy(sp).start()

    wd_start(1)

    depth = lax.broadcasted_iota(jnp.int32, (head_width, toks), 0)
    scale = half ** (-0.5)
    inputs[2].wait()
    split(2, store_rows)
    for h in range(heads):
        columns = turned(h) * scale
        qs[h, :, 0:toks] = jnp.where(depth < half, columns, 0.0).astype(BF16)
        qs[h, :, toks:] = jnp.where(depth >= half, columns, 0.0).astype(BF16)
    highs[...] = jnp.full_like(highs, -1e30)
    totals[...] = jnp.zeros_like(totals)
    acc[...] = jnp.zeros_like(acc)
    rows = lax.broadcasted_iota(jnp.int32, (toks, toks), 0)
    cols = lax.broadcasted_iota(jnp.int32, (toks, toks), 1)
    eye = rows == cols

    def process(b, masked):
        for h in range(heads):
            scores = mixed_dot(kall[b, head_rows(h), :], qs[h], ((1,), (0,)))
            if masked:
                scores = jnp.where(jnp.concatenate([rows <= cols] * 2, axis=1), scores, -1e30)
            old = highs[h]
            high = jnp.maximum(old, jnp.max(scores, axis=0, keepdims=True))
            shrink = jnp.exp(old - high)
            weights = jnp.exp(scores - high)
            totals[h] = shrink * totals[h] + jnp.sum(weights, axis=0, keepdims=True)
            blended = mixed_dot(
                vall[b, h * head_width : (h + 1) * head_width, :], weights.astype(BF16),
                ((1,), (0,)),
            )
            acc[h] = shrink * acc[h] + blended
            highs[h] = high

    with SC('proc_own'):
        process(sp, True)

    for load in small:
        load.wait()
    first = route_ref[0:1, :]
    lead = lax.broadcasted_iota(jnp.int32, (8, toks), 0)
    member = jnp.logical_and(
        first >= lead * per_group, first < (lead + 1) * per_group
    ).astype(F32)
    earlier = mixed_dot(member.astype(BF16), (rows < cols).astype(BF16), ((1,), (0,)))
    slot = jnp.sum(member * (earlier + lead.astype(F32) * cap), axis=0, keepdims=True)
    slot_col = jnp.sum(jnp.where(eye, slot, 0.0), axis=1, keepdims=True)
    slots = GROUPS * cap
    sel[...] = (
        lax.broadcasted_iota(jnp.int32, (slots, toks), 0) == slot.astype(jnp.int32)
    ).astype(BF16)
    selt[...] = (
        lax.broadcasted_iota(jnp.int32, (toks, slots), 1) == slot_col.astype(jnp.int32)
    ).astype(BF16)
    names = lax.broadcasted_iota(jnp.int32, (experts, toks), 0)
    by_expert = jnp.zeros((experts, toks), F32)
    for k in range(route_ref.shape[0]):
        by_expert = by_expert + jnp.where(
            names == route_ref[k : k + 1, :], rw_ref[k : k + 1, :], 0.0
        )
    by_slot = exact_pick(by_expert, selt[...])
    table = by_slot[:, 0:cap]
    for g in range(1, GROUPS):
        table = table + by_slot[:, g * cap : (g + 1) * cap]
    meta[sp, 0:experts, :] = table

    @pl.when(c == 1)
    def _():
        kv_sib_copy(2 * z).wait_recv()
        process(2 * z, False)

    def give_credits(j):
        def credit(which, plane):
            pl.semaphore_signal(
                free_sem.at[which], inc=1, device_id={"sp": 2 * plane + c, "tp": tp},
                device_id_type=MESH,
            )

        @pl.when(jnp.logical_and(j == z, z == zs - 2))
        def _():
            credit(0, 0)

        @pl.when(jnp.logical_and(j == z, z == zs - 1))
        def _():
            credit(1, 0)
            credit(1, 1)

    def visit(j, carry):
        b = 2 * (z - j) + c
        other = 2 * (z - j) + 1 - c
        with SC('wait_b'):
            kv_sib_copy(b).wait_recv()

        @pl.when(z < zs - 1)
        def _():
            next_copy(b).start()

        kv_sib_copy(b).start()
        give_credits(j)
        with SC('proc_b'):
            process(b, False)
        with SC('wait_o'):
            kv_sib_copy(other).wait_recv()
        with SC('proc_o'):
            process(other, False)
        return carry

    lax.fori_loop(1, z + 1, visit, 0)

    for h in range(heads):
        blend = acc[h] * (1.0 / totals[h])
        mix = blend[:, :toks] - lam_ref[:, h : h + 1] * blend[:, toks:]
        mix = mix * lax.rsqrt(jnp.mean(mix * mix, axis=0, keepdims=True) + norm_eps)
        att[:, h * head_width : (h + 1) * head_width] = (mix.T * gain_ref[...]).astype(BF16)
    inputs[3].wait()

    def projected(to):
        return jnp.dot(
            att[...], owv[:, pl.ds(pl.multiple_of(to * piece, piece), piece)],
            preferred_element_type=F32,
        )

    half_toks = toks // 2
    part_halves = (slice(0, half_toks), slice(half_toks, toks))

    def rs_copy(i):
        to, source, target = [
            (beside, part.at[across, part_halves[0]], ppass.at[0]),
            (above, part.at[across, part_halves[1]], ppass.at[1]),
            (beside, part.at[beside, part_halves[0]], rbuf.at[0, part_halves[0]]),
            (above, part.at[above, part_halves[1]], rbuf.at[1, part_halves[1]]),
            (above, part.at[above, part_halves[0]], rbuf.at[1, part_halves[0]]),
            (beside, part.at[beside, part_halves[1]], rbuf.at[0, part_halves[1]]),
        ][i]
        return remote(source, target, rs_send, rs_recv.at[min(i, 2)], sp, to)

    part[across] = projected(across).astype(BF16)
    rs_copy(0).start()
    rs_copy(1).start()
    for_beside = projected(beside)
    part[beside, part_halves[0]] = for_beside[part_halves[0]].astype(BF16)
    rs_copy(2).start()
    for_above = projected(above)
    part[above, part_halves[1]] = for_above[part_halves[1]].astype(BF16)
    rs_copy(3).start()
    mine = pl.ds(pl.multiple_of(tp * piece, piece), piece)
    inputs[4].wait()
    total = resv[:, mine].astype(F32) + projected(tp)
    with SC("rs_pass"):
        rs_copy(0).wait_recv()
    part[above, part_halves[0]] = (for_above[part_halves[0]] + ppass[0].astype(F32)).astype(BF16)
    rs_copy(4).start()
    with SC("rs_pass"):
        rs_copy(1).wait_recv()
    part[beside, part_halves[1]] = (for_beside[part_halves[1]] + ppass[1].astype(F32)).astype(BF16)
    rs_copy(5).start()
    wd_start(2)

    half_cap = cap // 2

    def spot(src, core, part):
        return xall.at[
            src,
            pl.ds(pl.multiple_of(core * cap, cap), cap),
            pl.ds(pl.multiple_of(part * piece, piece), piece),
        ]

    def half_spot(src, part, side):
        return xall.at[
            src,
            pl.ds(pl.multiple_of(c * cap + side * half_cap, half_cap), half_cap),
            pl.ds(pl.multiple_of(part * piece, piece), piece),
        ]

    def x_copy(s):
        group = (z + s) % zs
        return remote(
            xs.at[s], spot(z, c, tp), x_send, x_recv.at[z, 0], 2 * group + c, tp
        )

    def spot_wait(here, sem):
        remote(here, here, x_send, sem, sib, tp).wait_recv()

    def tp_copy(src, i):
        to, side = [(beside, 0), (above, 1), (beside, 1), (above, 0)][i]
        here = half_spot(src, tp, side)
        return remote(here, here, x_tp, x_recv.at[src, 1 + i // 2], sp, to)

    def pass_copy(src, i):
        part, side, to = [(beside, 0, above), (above, 1, beside)][i]
        here = half_spot(src, part, side)
        return remote(here, here, x_tp, x_recv.at[src, 3], sp, to)

    def sib_copy(src, part):
        here = spot(src, c, part)
        return remote(here, here, x_sib, s_recv.at[src], sib, tp)

    def gather(src):
        @pl.when(src != z)
        def _():
            with SC("arrive"):
                spot_wait(spot(src, c, tp), x_recv.at[src, 0])

        for i in range(4):
            tp_copy(src, i).start()
        sib_copy(src, tp).start()

    def gather_pass(src):
        with SC("gpass"):
            spot_wait(spot(src, c, beside), x_recv.at[src, 1])
        pass_copy(src, 0).start()
        pass_copy(src, 1).start()

    def forward(src):
        with SC("compl_tp"):
            spot_wait(spot(src, c, beside), x_recv.at[src, 2])
            sib_copy(src, beside).start()
            sib_copy(src, above).start()
            spot_wait(spot(src, c, across), x_recv.at[src, 3])
            sib_copy(src, across).start()

    def complete(src):
        with SC("compl_sib"):
            spot_wait(
                xall.at[src, pl.ds(pl.multiple_of((1 - c) * cap, cap), cap)], s_recv.at[src]
            )

    pl.when(z > 0)(lambda: gather(0))
    pl.when(z == zs - 2)(lambda: gather(1))

    with SC("rs_wait"):
        remote(rbuf, rbuf, rs_send, rs_recv.at[2], sp, beside).wait_recv()
    total = total + rbuf[0].astype(F32) + rbuf[1].astype(F32)
    stream_ref[...] = total
    normed_ref[...] = (total * fg_ref[:, mine]).astype(BF16)
    squares = jnp.sum(total * total, axis=1, keepdims=True)
    as_row = jnp.sum(jnp.where(eye, squares, 0.0), axis=0, keepdims=True)
    sq_send[...] = jnp.broadcast_to(as_row, sq_send.shape)

    def sq_copy(d):
        return remote(
            sq_send, sq_recv.at[d], sq_ss, sq_rs, sp, (tp + d) % tps
        )

    for d in range(1, tps):
        sq_copy(d).start()

    def m_copy(d):
        return remote(meta.at[sp], meta.at[sp], m_send, m_recv.at[sp], (sp + d) % n, tp)

    def m_wait(src):
        @pl.when(src != sp)
        def _():
            remote(meta.at[src], meta.at[src], m_send, m_recv.at[src], sib, tp).wait_recv()

    for s in list(range(1, zs)) + [0]:
        group = (z + s) % zs
        picked = jnp.dot(
            sel[pl.ds(pl.multiple_of(group * cap, cap), cap), :], normed_ref[...],
            preferred_element_type=F32,
        ).astype(BF16)
        if s:
            xs[s] = picked
            pl.when(z >= (zs - s if s >= zs - 2 else 0))(lambda: x_copy(s).start())
        else:
            spot(z, c, tp)[...] = picked

    @pl.when(z < zs - 1)
    def _():
        gather(z)

    wd_start(3)

    def row_factors():
        with SC("sq_wait"):
            squares_in = sq_recv.at[pl.ds(1, tps - 1)]
            remote(squares_in, squares_in, sq_ss, sq_rs, sp, beside).wait_recv()
        sums = sq_send[0:1, :]
        for d in range(1, tps):
            sums = sums + sq_recv[d, 0:1, :]
        inverse = lax.rsqrt(sums * (1.0 / (piece * tps)) + norm_eps)
        by_slot = exact_pick(jnp.broadcast_to(inverse, (8, toks)), selt[...])
        for g in range(GROUPS):
            meta[sp, experts + g : experts + g + 1, :] = by_slot[0:1, g * cap : (g + 1) * cap]
        for d in range(1, n):
            m_copy(d).start()

    def late_rows(s, which):
        with SC("credit"):
            pl.semaphore_wait(free_sem.at[which], 1)
        x_copy(s).start()

    pl.when(z < zs - 2)(row_factors)
    gather_pass(0)

    @pl.when(z == zs - 2)
    def _():
        gather_pass(1)
        gather_pass(2)

    pl.when(z == zs - 1)(lambda: gather(1))
    wd_start(4)
    pl.when(z == zs - 2)(row_factors)
    pl.when(z == 1)(lambda: late_rows(zs - 2, 1))

    @pl.when(z == 0)
    def _():
        late_rows(zs - 2, 0)
        gather(1)
        late_rows(zs - 1, 1)

    def late_sources():
        gather(zs - 2)
        pl.when(z == 0)(lambda: gather_pass(1))
        wd_start(5)
        forward(1)
        gather_pass(zs - 2)
        wd_start(6)

    def near_copy(src, part):
        return remote(
            away.at[src, part], near.at[src, part], n_send,
            n_recv.at[src, jnp.where(part == across, 0, 1)], sib, tp,
        )

    def near_wait(src, first):
        here = near.at[src, pl.ds(0, 1 if first else tps - 1)]
        remote(here, here, n_send, n_recv.at[src, 0 if first else 1], sib, tp).wait_recv()

    tile = 512
    small_eye = lax.broadcasted_iota(jnp.int32, (cap, cap), 0) == lax.broadcasted_iota(
        jnp.int32, (cap, cap), 1
    )
    which = lax.broadcasted_iota(jnp.int32, meta.shape[1:], 0)

    def meta_col(src, core, line):
        row = jnp.sum(jnp.where(which == line, meta[2 * src + core], 0.0), axis=0, keepdims=True)
        return jnp.sum(jnp.where(small_eye, row, 0.0), axis=1, keepdims=True)

    keep_rows = pl.ds(pl.multiple_of(c * cap, cap), cap)
    away_rows = pl.ds(pl.multiple_of((1 - c) * cap, cap), cap)

    def ffn_one(src, between):
        @pl.when(src == 0)
        def _():
            for load in loads:
                load.wait()

        with SC("m_wait"):
            m_wait(2 * src)
            m_wait(2 * src + 1)
        factor = jnp.concatenate(
            [meta_col(src, c, experts + z), meta_col(src, 1 - c, experts + z)], axis=0
        )

        def one(i, carry):
            pl.when(i == wg.shape[1] // tile // 2)(between)
            at = pl.ds(pl.multiple_of(i * tile, tile), tile)
            x = jnp.concatenate([xall[src, keep_rows], xall[src, away_rows]], axis=0)
            gate = jnp.dot(x, wg[:, at], preferred_element_type=F32) * factor
            up = jnp.dot(x, wu[:, at], preferred_element_type=F32) * factor
            hid[src, :, at] = (gate / (1.0 + jnp.exp(-gate)) * up).astype(BF16)
            return carry

        with SC("ffn_one"):
            lax.fori_loop(0, wg.shape[1] // tile, one, 0)

    def ffn_two(src, first):
        @pl.when(first)
        def _():
            with SC("down_wait"):
                others = wdv.at[pl.ds(0, tps - 1)]
                remote(others, others, wd_send, wd_recv, sp, beside).wait()

        row_weight = jnp.concatenate(
            [meta_col(src, c, sp), meta_col(src, 1 - c, sp)], axis=0
        )

        def two(j, carry):
            to = tp ^ (tps - 1 - j)
            result = jnp.dot(hid[src], wdv[to], preferred_element_type=F32) * row_weight
            away[src, to] = result[cap:].astype(BF16)
            near_copy(src, to).start()
            keep[src, to] = result[:cap]
            return carry

        with SC("ffn_two"):
            lax.fori_loop(0, tps, two, 0)

    cap_halves = (slice(0, half_cap), slice(half_cap, cap))

    def r_copy(src, i):
        to, source, target = [
            (beside, rsend.at[src, across, cap_halves[0]], rpass.at[src, 0]),
            (above, rsend.at[src, across, cap_halves[1]], rpass.at[src, 1]),
            (beside, rsend.at[src, beside, cap_halves[0]], rrecv.at[src, 0, cap_halves[0]]),
            (above, rsend.at[src, above, cap_halves[1]], rrecv.at[src, 1, cap_halves[1]]),
            (above, rsend.at[src, above, cap_halves[0]], rrecv.at[src, 1, cap_halves[0]]),
            (beside, rsend.at[src, beside, cap_halves[1]], rrecv.at[src, 0, cap_halves[1]]),
        ][i]
        return remote(source, target, r_send, r_recv.at[src, min(i // 2, 1)], sp, to)

    def both(src, to, at):
        return keep[src, to, at, :] + near[src, to, at, :].astype(F32)

    def spread(src):
        with SC("near_wait"):
            near_wait(src, True)
        rsend[src, across] = both(src, across, slice(0, cap)).astype(BF16)
        r_copy(src, 0).start()
        r_copy(src, 1).start()
        near_wait(src, False)
        rsend[src, above, cap_halves[1]] = both(src, above, cap_halves[1]).astype(BF16)
        r_copy(src, 3).start()
        rsend[src, beside, cap_halves[0]] = both(src, beside, cap_halves[0]).astype(BF16)
        r_copy(src, 2).start()

    def spread_pass(src):
        with SC("spass"):
            passed = rpass.at[src]
            remote(passed, passed, r_send, r_recv.at[src, 0], sp, beside).wait_recv()
        rsend[src, above, cap_halves[0]] = (
            both(src, above, cap_halves[0]) + rpass[src, 0].astype(F32)
        ).astype(BF16)
        r_copy(src, 4).start()
        rsend[src, beside, cap_halves[1]] = (
            both(src, beside, cap_halves[1]) + rpass[src, 1].astype(F32)
        ).astype(BF16)
        r_copy(src, 5).start()

    def b_copy(src):
        return remote(
            back.at[src], ret.at[z], b_send, b_recv, 2 * src + c, tp
        )

    def finish(src):
        with SC("r_wait"):
            here = rrecv.at[src]
            remote(here, here, r_send, r_recv.at[src, 1], sp, beside).wait_recv()
        total = both(src, tp, slice(0, cap))
        total = total + rrecv[src, 0].astype(F32) + rrecv[src, 1].astype(F32)

        @pl.when(src == z)
        def _():
            ret[z] = total.astype(BF16)

        @pl.when(src != z)
        def _():
            back[src] = total.astype(BF16)
            b_copy(src).start()

    last = zs - 1

    at_last = z == last

    early = z < last

    def when_both(one, two):
        return pl.when(jnp.logical_and(one, two))

    third = z == last - 1
    first_two = z < last - 1
    lead = jnp.where(first_two, last - 1, 0)
    after = jnp.where(z == 1, 0, 1)

    def up_step(s):
        def between():
            when_both(third, s == 0)(lambda: forward(1))
            when_both(z == 1, s == 0)(lambda: gather_pass(1))
            when_both(early, s == 1)(lambda: forward(2))
            when_both(early, s == last - 1)(lambda: gather(last))
            when_both(early, s == last)(lambda: finish(lead))
            when_both(early, s == last)(lambda: spread_pass(after))
            when_both(at_last, s < last)(lambda: gather_pass(s + 1))
            when_both(at_last, s + 2 <= last)(lambda: gather(s + 2))

        pl.when(s == 0)(lambda: forward(0))
        when_both(at_last, s == 0)(row_factors)
        when_both(first_two, s == 1)(late_sources)
        complete(s)
        ffn_one(s, between)
        when_both(at_last, s == last)(lambda: spread_pass(last - 1))

    def down_step(s):
        ffn_two(s, s == jnp.where(early, lead, 0))
        when_both(at_last, s < last)(lambda: forward(s + 1))
        when_both(early, s == lead)(lambda: gather_pass(last))
        when_both(early, s == after)(lambda: spread_pass(lead))
        when_both(early, s == z)(lambda: spread_pass(last))
        when_both(at_last, jnp.logical_and(s >= 1, s < last))(lambda: spread_pass(s - 1))
        spread(s)
        when_both(early, s == after)(lambda: forward(last))
        when_both(early, s == last)(lambda: finish(after))
        when_both(at_last, s == last - 1)(lambda: finish(0))

        @pl.when(jnp.logical_and(at_last, s == last))
        def _():
            finish(1)
            finish(2)

    def step(k, carry):
        turn = k
        for at, value in enumerate(
            (0, 2, 4, 2 * lead + 1, 2 * after + 1, 2 * last, 2 * last + 1, 2 * z + 1)
        ):
            turn = jnp.where(jnp.logical_and(early, k == at), value, turn)
        pl.when(turn % 2 == 0)(lambda: up_step(turn // 2))
        pl.when(turn % 2 == 1)(lambda: down_step(turn // 2))
        return carry

    lax.fori_loop(0, 2 * zs, step, 0)
    pl.when(at_last)(lambda: spread_pass(last))
    finish(last)

    @pl.when(early)
    def _():
        spread_pass(z)
        finish(z)

    with SC("b_wait"):
        returns = ret.at[pl.ds(0, zs - 1)]
        remote(returns, returns, b_send, b_recv, sib, tp).wait_recv()
    rows = ret[...].reshape(zs * cap, piece)
    layer = stream_ref[...] + jnp.dot(selt[...], rows, preferred_element_type=F32)
    outv[:, mine] = layer.astype(BF16)

    def out_spot(part, side):
        return outv.at[part_halves[side], pl.ds(pl.multiple_of(part * piece, piece), piece)]

    def o_copy(i):
        part, side, to = [
            (tp, 0, beside), (tp, 1, above), (tp, 1, beside), (tp, 0, above),
            (beside, 0, above), (above, 1, beside),
        ][i]
        here = out_spot(part, side)
        return remote(here, here, o_send, o_recv.at[min(i, 4)], sp, to)

    def o_wait(part, i, side=None):
        at = pl.ds(pl.multiple_of(part * piece, piece), piece)
        here = outv.at[:, at] if side is None else out_spot(part, side)
        remote(here, here, o_send, o_recv.at[i], sib, tp).wait_recv()

    for i in range(4):
        o_copy(i).start()
    with SC("o_pass"):
        o_wait(beside, 0, 0)
    o_copy(4).start()
    with SC("o_pass"):
        o_wait(above, 1, 1)
    o_copy(5).start()

    def sent(here, sem):
        remote(here, here, sem, kv_recv.at[0], sib, tp).wait_send()

    sent(sq_recv.at[pl.ds(1, tps - 1)], sq_ss)
    sent(part.at[pl.ds(0, 3)], rs_send)
    sent(meta.at[pl.ds(0, n - 1)], m_send)
    sent(xs.at[pl.ds(1, zs - 1)], x_send)
    sent(back.at[pl.ds(0, zs - 1)], b_send)
    sent(away, n_send)
    sent(away, x_sib)
    sent(away.at[pl.ds(0, zs - 1)], x_tp)
    sent(away.at[pl.ds(0, zs - 1)], r_send)

    @pl.when(z < zs - 1)
    def _():
        next_copy(sp).wait_send()

    @pl.when(c == 0)
    def _():
        kv_sib_copy(sp).wait_send()

    def drain(j, carry):
        b = 2 * (z - j) + c

        @pl.when(z < zs - 1)
        def _():
            next_copy(b).wait_send()

        kv_sib_copy(b).wait_send()
        return carry

    lax.fori_loop(1, z + 1, drain, 0)
    with SC("o_wait"):
        o_wait(beside, 2, 1)
        o_wait(above, 3, 0)
        o_wait(across, 4)
    with SC("o_send"):
        sent(part.at[pl.ds(0, 3)], o_send)


def paired_shards(
    residual, queries, key_vectors, value_rows, head_lambda, head_gain, out_weight, ffn_gain,
    expert_gate, expert_up, expert_down, routing, route_weight,
):
    n = lax.axis_size("sp")
    tps = lax.axis_size("tp")
    toks, heads, head_width = queries.shape
    width = heads * head_width
    model = residual.shape[1]
    piece = model // tps
    experts = n
    per_group = experts // GROUPS
    cap = toks // per_group
    down = expert_down[0]
    wd_rows = down.shape[0] // tps
    vmem = pl.BlockSpec(memory_space=pltpu.VMEM)
    hbm = pl.BlockSpec(memory_space=pltpu.HBM)
    dma = pltpu.SemaphoreType.DMA
    zs = n // 2
    def stay(x):
        return pltpu.with_memory_space_constraint(x, pltpu.HBM)

    return pl.pallas_call(
        functools.partial(layer_kernel, n, tps, cap, heads, head_width),
        out_shape=jax.ShapeDtypeStruct((toks, model), BF16),
        in_specs=[hbm] * 13,
        out_specs=vmem,
        scratch_shapes=[
            pltpu.VMEM(routing.shape[::-1], jnp.int32),
            pltpu.VMEM(route_weight.shape[::-1], F32),
            pltpu.VMEM((1, heads), F32),
            pltpu.VMEM((1, head_width), F32),
            pltpu.VMEM((1, model), F32),
            pltpu.VMEM((3, toks * heads, head_width), BF16),
            pltpu.VMEM((toks, model), BF16),
            pltpu.VMEM((width, model), BF16),
            pltpu.VMEM((GROUPS * cap, toks), BF16),
            pltpu.VMEM((toks, GROUPS * cap), BF16),
            pltpu.VMEM((toks, piece), F32),
            pltpu.VMEM((toks, piece), BF16),
            pltpu.VMEM((n, experts + 8, cap), F32),
            pltpu.VMEM((zs, cap, piece), BF16),
            pltpu.VMEM((zs, 2 * cap, model), BF16),
            pltpu.VMEM(expert_gate.shape[1:], BF16),
            pltpu.VMEM(expert_up.shape[1:], BF16),
            pltpu.VMEM((tps, wd_rows, piece), BF16),
            pltpu.VMEM((zs, 2 * cap, expert_gate.shape[2]), BF16),
            pltpu.VMEM((zs, tps, cap, piece), F32),
            pltpu.VMEM((zs, tps, cap, piece), BF16),
            pltpu.VMEM((zs, tps, cap, piece), BF16),
            pltpu.VMEM((zs, tps, cap, piece), BF16),
            pltpu.VMEM((zs, 2, cap, piece), BF16),
            pltpu.VMEM((zs, 2, cap // 2, piece), BF16),
            pltpu.VMEM((zs, cap, piece), BF16),
            pltpu.VMEM((zs, cap, piece), BF16),
            pltpu.VMEM((n, heads * toks, head_width), BF16),
            pltpu.VMEM((n, width, toks), BF16),
            pltpu.VMEM((heads * toks, head_width), BF16),
            pltpu.VMEM((heads, head_width, 2 * toks), BF16),
            pltpu.VMEM((heads, 1, 2 * toks), F32),
            pltpu.VMEM((heads, 1, 2 * toks), F32),
            pltpu.VMEM((heads, head_width, 2 * toks), F32),
            pltpu.VMEM((toks, width), BF16),
            pltpu.VMEM((tps, toks, piece), BF16),
            pltpu.VMEM((2, toks, piece), BF16),
            pltpu.VMEM((2, toks // 2, piece), BF16),
            pltpu.VMEM((8, toks), F32),
            pltpu.VMEM((tps, 8, toks), F32),
            dma((10,)), dma((3,)),
            dma, dma, dma, dma((zs, 4)), dma((zs,)),
            dma, dma((zs, 2)), dma, dma((zs, 2)),
            dma, dma, dma, dma((5,)),
            dma((zs,)), dma((zs,)), dma((n,)),
            dma, dma, dma, dma((n,)),
            dma, dma((3,)), dma, dma, pltpu.SemaphoreType.REGULAR((2,)),
        ],
        compiler_params=pltpu.CompilerParams(collective_id=0, has_side_effects=True, vmem_limit_bytes=49545216),
        name="layer",
    )(
        stay(queries.reshape(toks * heads, head_width)), stay(key_vectors.reshape(toks * heads, head_width)),
        stay(value_rows.reshape(toks * heads, head_width)), stay(routing.T), stay(route_weight.T), stay(down),
        stay(head_lambda.reshape(1, -1)), stay(head_gain.reshape(1, -1)), stay(out_weight), stay(residual), stay(ffn_gain.reshape(1, -1)),
        stay(expert_gate), stay(expert_up),
    )


def solution(mesh):
    in_specs = (
        P("sp", None),
        P("sp", "tp", None),
        P("sp", "tp", None),
        P("sp", "tp", None),
        P("tp"),
        P(),
        P("tp", None),
        P(),
        P("sp", None, "tp"),
        P("sp", None, "tp"),
        P("sp", None, "tp"),
        P("sp", None),
        P("sp", None),
    )
    out_specs = P("sp", None)
    paired = mesh.shape["sp"] == 2 * GROUPS and mesh.shape["tp"] == 4
    return jax.shard_map(paired_shards if paired else shards, mesh=mesh, in_specs=in_specs, out_specs=out_specs, check_vma=False)
```

```python
import functools
import math

import jax
import jax.numpy as jnp
from jax import lax
from jax.experimental import pallas as pl
from jax.experimental.pallas import tpu as pltpu
from jax.sharding import PartitionSpec as P

GROUPS = 4
SC = jax.named_scope


norm_eps = 1e-06


def online_update(running, query_part, key_part, value_part, query_pos, key_pos, score_scale):
    highest, totals, accum = running
    scores = (
        jnp.einsum("qhd,khd->hqk", query_part, key_part, preferred_element_type=jnp.float32)
        * score_scale
    )
    scores = jnp.where(key_pos[None, None, :] <= query_pos[None, :, None], scores, -jnp.inf)
    new_high = jnp.maximum(highest, jnp.max(scores, axis=-1))
    shrink = jnp.exp(highest - new_high)
    weights = jnp.exp(scores - new_high[:, :, None])
    totals = shrink * totals + jnp.sum(weights, axis=-1)
    blended = jnp.einsum(
        "hqk,khe->qhe", weights.astype(jnp.bfloat16), value_part, preferred_element_type=jnp.float32
    )
    accum = jnp.transpose(shrink)[:, :, None] * accum + blended
    return (new_high, totals, accum)


def shards(
    residual,
    queries,
    key_vectors,
    value_rows,
    head_lambda,
    head_gain,
    out_weight,
    ffn_gain,
    expert_gate,
    expert_up,
    expert_down,
    routing,
    route_weight,
):
    tok_count = queries.shape[0]
    local_heads = queries.shape[1]
    half_width = queries.shape[2] // 2
    value_width = value_rows.shape[2]
    score_scale = half_width ** (-0.5)
    query_pos = lax.axis_index("sp") * tok_count + jnp.arange(tok_count, dtype=jnp.int32)
    last_query = query_pos[-1]
    first_half = queries[:, :, :half_width]
    second_half = queries[:, :, half_width:]
    start_high = jnp.full((local_heads, tok_count), -1e30, jnp.float32)
    start_total = jnp.zeros((local_heads, tok_count), jnp.float32)
    start_accum = jnp.zeros((tok_count, local_heads, value_width), jnp.float32)
    empty_state = (start_high, start_total, start_accum)
    running = (empty_state, empty_state)
    key_piece = lax.all_gather(key_vectors, "sp", axis=0, tiled=True)
    value_piece = lax.all_gather(value_rows, "sp", axis=0, tiled=True)
    piece_len = key_piece.shape[0]
    block_len = math.gcd(piece_len, 512)
    block_count = piece_len // block_len
    key_blocks = key_piece.reshape(block_count, block_len, local_heads, 2 * half_width)
    value_blocks = value_piece.reshape(block_count, block_len, local_heads, value_width)

    def visit(current, stacked):
        block_index, key_block, value_block = stacked
        block_first = block_index * block_len
        key_pos = block_first + jnp.arange(block_len, dtype=jnp.int32)

        def compute(inside):
            first_state = online_update(
                inside[0],
                first_half,
                key_block[:, :, :half_width],
                value_block,
                query_pos,
                key_pos,
                score_scale,
            )
            second_state = online_update(
                inside[1],
                second_half,
                key_block[:, :, half_width:],
                value_block,
                query_pos,
                key_pos,
                score_scale,
            )
            return (first_state, second_state)

        return (lax.cond(block_first <= last_query, compute, lambda inside: inside, current), None)

    running, _ = lax.scan(
        visit, running, (jnp.arange(block_count, dtype=jnp.int32), key_blocks, value_blocks)
    )
    first_state, second_state = running
    first_out = first_state[2] / jnp.transpose(first_state[1])[:, :, None]
    second_out = second_state[2] / jnp.transpose(second_state[1])[:, :, None]
    combined = first_out - head_lambda[None, :, None] * second_out
    normed_heads = (
        combined
        * lax.rsqrt(jnp.mean(combined * combined, axis=-1, keepdims=True) + norm_eps)
        * head_gain
    )
    attended = normed_heads.astype(jnp.bfloat16).reshape(tok_count, local_heads * value_width)
    partial_proj = jnp.dot(attended, out_weight, preferred_element_type=jnp.float32)
    projected = lax.psum(partial_proj.astype(jnp.bfloat16), "tp").astype(jnp.float32)
    stream = residual.astype(jnp.float32) + projected
    block_normed = (
        stream * lax.rsqrt(jnp.mean(stream * stream, axis=-1, keepdims=True) + norm_eps) * ffn_gain
    ).astype(jnp.bfloat16)
    expert_count = lax.axis_size("sp")
    tp_count = lax.axis_size("tp")
    per_group = expert_count // GROUPS
    capacity = tok_count // per_group
    top_count = routing.shape[1]
    model_width = block_normed.shape[1]
    flat_routes = routing.reshape(-1)
    route_count = flat_routes.shape[0]
    onehot = (flat_routes[:, None] == jnp.arange(expert_count, dtype=jnp.int32)[None, :]).astype(
        jnp.int32
    )
    earlier = jnp.cumsum(onehot, axis=0) - onehot
    position = jnp.sum(earlier * onehot, axis=1)
    slot_index = flat_routes * capacity + position
    slot_token = (
        jnp.full((expert_count * capacity,), tok_count, jnp.int32)
        .at[slot_index]
        .set(jnp.arange(route_count, dtype=jnp.int32) // top_count)
    )
    slot_table = slot_token.reshape(expert_count, capacity)
    slice_width = model_width // tp_count
    own_columns = lax.dynamic_slice_in_dim(
        block_normed, lax.axis_index("tp") * slice_width, slice_width, 1
    )
    outgoing = jnp.take(own_columns, slot_table, axis=0, mode="fill", fill_value=0)
    landed = lax.all_to_all(outgoing, "sp", split_axis=0, concat_axis=0, tiled=True)
    arrived = lax.all_gather(landed, "tp", axis=2, tiled=True)
    expert_rows = arrived.reshape(-1, model_width)
    gate_part = jnp.dot(expert_rows, expert_gate[0], preferred_element_type=jnp.float32)
    up_part = jnp.dot(expert_rows, expert_up[0], preferred_element_type=jnp.float32)
    inner_act = (jax.nn.silu(gate_part) * up_part).astype(jnp.bfloat16)
    down_width = expert_down.shape[2]
    weight_rows = expert_down[0]
    expert_sum = jnp.dot(
        lax.all_gather(inner_act, "tp", axis=1, tiled=True),
        weight_rows,
        preferred_element_type=jnp.float32,
    )
    expert_out = expert_sum.astype(jnp.bfloat16).reshape(expert_count, capacity, down_width)
    returned = lax.all_to_all(expert_out, "sp", split_axis=0, concat_axis=0, tiled=True)
    per_route = returned.reshape(expert_count * capacity, down_width)[slot_index]
    weighted = per_route.astype(jnp.float32) * route_weight.reshape(-1)[:, None]
    token_sum = jnp.sum(weighted.reshape(tok_count, top_count, down_width), axis=1)
    moe_rows = lax.all_gather(token_sum.astype(jnp.bfloat16), "tp", axis=1, tiled=True).astype(
        token_sum.dtype
    )
    return (stream + moe_rows).astype(jnp.bfloat16)


MESH = pl.DeviceIdType.MESH
F32 = jnp.float32
BF16 = jnp.bfloat16


def remote(src, dst, send_sem, recv_sem, sp, tp):
    return pltpu.make_async_remote_copy(
        src_ref=src,
        dst_ref=dst,
        send_sem=send_sem,
        recv_sem=recv_sem,
        device_id={"sp": sp, "tp": tp},
        device_id_type=MESH,
    )


def mixed_dot(left, right, contract):
    return lax.dot_general(left, right, (contract, ((), ())), preferred_element_type=F32)


def dispersed(value):
    high = value.astype(BF16)
    rest = value - high.astype(F32)
    middle = rest.astype(BF16)
    low = (rest - middle.astype(F32)).astype(BF16)
    return jnp.concatenate([high, middle, low], axis=0)


def exact_pick(value, picker):
    count = value.shape[0]
    parts = mixed_dot(dispersed(value), picker, ((1,), (0,)))
    return parts[:count] + parts[count : 2 * count] + parts[2 * count :]


def layer_kernel(
    n, tps, cap, heads, head_width,
    q_ref, k_ref, v_ref, route_in, rw_in, wd_ref, lam_in, gain_in, ow_ref, res_ref, fg_in,
    gate_ref, up_ref,
    outv,
    route_ref, rw_ref, lam_ref, gain_ref, fg_ref, raw, resv, owv, sel, selt, stream_ref, normed_ref, meta,
    xs, xall, wg, wu, wdv, hid, keep, away, near, rsend, rrecv, rpass, back, ret,
    kall, vall, rowm, qs, highs, totals, acc, att, part, rbuf, ppass, sq_send, sq_recv,
    in_sem, w_sem, x_send, x_tp, x_sib, x_recv, s_recv, n_send, n_recv, r_send, r_recv,
    b_send, b_recv, o_send, o_recv,
    kv_next, kv_sib, kv_recv, wd_send, wd_recv, m_send, m_recv,
    rs_send, rs_recv, sq_ss, sq_rs, free_sem,
):
    sp = lax.axis_index("sp")
    tp = lax.axis_index("tp")
    z, c = sp // 2, sp % 2
    zs = n // 2
    sib = 2 * z + 1 - c
    toks = resv.shape[0]
    width = heads * head_width
    half = head_width // 2
    piece = normed_ref.shape[1]
    wd_rows = wdv.shape[1]
    experts = n
    per_group = experts // GROUPS
    beside, above, across = tp ^ 1, tp ^ 2, tp ^ 3

    barrier = pltpu.get_barrier_semaphore()
    for d in range(1, n):
        pl.semaphore_signal(
            barrier, inc=1, device_id={"sp": (sp + d) % n, "tp": tp}, device_id_type=MESH
        )
    for d in range(1, tps):
        pl.semaphore_signal(
            barrier, inc=1, device_id={"sp": sp, "tp": (tp + d) % tps}, device_id_type=MESH
        )
    inputs = [
        pltpu.make_async_copy(k_ref, raw.at[0], in_sem.at[0]),
        pltpu.make_async_copy(v_ref, raw.at[1], in_sem.at[1]),
        pltpu.make_async_copy(q_ref, raw.at[2], in_sem.at[2]),
        pltpu.make_async_copy(ow_ref, owv, in_sem.at[3]),
        pltpu.make_async_copy(res_ref, resv, in_sem.at[4]),
    ]
    small = [
        pltpu.make_async_copy(given, kept, in_sem.at[5 + i])
        for i, (given, kept) in enumerate(
            (
                (route_in, route_ref), (rw_in, rw_ref), (lam_in, lam_ref), (gain_in, gain_ref),
                (fg_in, fg_ref),
            )
        )
    ]
    loads = [
        pltpu.make_async_copy(gate_ref.at[0], wg, w_sem.at[0]),
        pltpu.make_async_copy(up_ref.at[0], wu, w_sem.at[1]),
        pltpu.make_async_copy(
            wd_ref.at[pl.ds(pl.multiple_of(tp * wd_rows, wd_rows), wd_rows), :],
            wdv.at[tp], w_sem.at[2],
        ),
    ]
    for load in inputs + small + loads:
        load.start()

    run = toks // heads
    spot_row = lax.broadcasted_iota(jnp.int32, (run, toks), 0)
    spot_col = lax.broadcasted_iota(jnp.int32, (run, toks), 1)
    order = jnp.concatenate(
        [(spot_col == spot_row * heads + h).astype(BF16) for h in range(heads)], axis=0
    )

    def split(which, store):
        for i in range(heads):
            rows = jnp.dot(
                order, raw[which, i * toks : (i + 1) * toks, :], preferred_element_type=F32
            )
            for h in range(heads):
                store(i, h, rows[h * run : (h + 1) * run, :])

    def head_rows(h, i=0, count=toks):
        return slice(h * toks + i * run, h * toks + i * run + count)

    def store_keys(i, h, rows):
        kall[sp, head_rows(h, i, run), :] = rows.astype(BF16)

    def store_rows(i, h, rows):
        rowm[head_rows(h, i, run), :] = rows.astype(BF16)

    unit = (
        lax.broadcasted_iota(jnp.int32, (head_width, head_width), 0)
        == lax.broadcasted_iota(jnp.int32, (head_width, head_width), 1)
    ).astype(BF16)

    def turned(h):
        return mixed_dot(unit, rowm[head_rows(h), :], ((1,), (1,)))

    inputs[0].wait()
    split(0, store_keys)
    inputs[1].wait()
    split(1, store_rows)
    for h in range(heads):
        vall[sp, h * head_width : (h + 1) * head_width, :] = turned(h).astype(BF16)

    chunks = 8
    wd_run = wd_rows // chunks

    def wd_copy(k, d):
        to = tp ^ d
        return remote(
            wd_ref.at[pl.ds(pl.multiple_of(to * wd_rows + k * wd_run, wd_run), wd_run), :],
            wdv.at[tp, pl.ds(pl.multiple_of(k * wd_run, wd_run), wd_run)],
            wd_send, wd_recv, sp, to,
        )

    def by_plane(values):
        chosen = values[-1]
        for plane, value in enumerate(values[:-1]):
            chosen = jnp.where(z == plane, value, chosen)
        return chosen

    wd_points = [
        (0, 0, 0, 0), (1, 3, 5, 7), (2, 4, 6, 7), (3, 4, 6, 7), (6, 6, 8, 8), (7, 7, 8, 8), (8, 8, 8, 8)
    ]

    def wd_start(point):
        def start(k, carry):
            for d in (3, 1, 2):
                wd_copy(k, d).start()
            return carry

        lax.fori_loop(by_plane(wd_points[point - 1]), by_plane(wd_points[point]), start, 0)

    class KeyCopies:
        def __init__(self, b, sends, to):
            self.at = (sends.at[b // 2], kv_recv.at[b], to, tp)
            self.block = b

        def start(self):
            for blocks in (kall, vall):
                here = blocks.at[self.block]
                remote(here, here, *self.at).start()

        def wait_send(self):
            both = kall.at[pl.ds(0, 2)]
            remote(both, both, *self.at).wait_send()

        def wait_recv(self):
            both = kall.at[pl.ds(0, 2)]
            remote(both, both, *self.at).wait_recv()

    def next_copy(b):
        return KeyCopies(b, kv_next, sp + 2)

    def kv_sib_copy(b):
        return KeyCopies(b, kv_sib, sib)

    with SC('barrier_wait'):
        pl.semaphore_wait(barrier, n - 1 + tps - 1)

    @pl.when(z < zs - 1)
    def _():
        next_copy(sp).start()

    @pl.when(c == 0)
    def _():
        kv_sib_copy(sp).start()

    wd_start(1)

    depth = lax.broadcasted_iota(jnp.int32, (head_width, toks), 0)
    scale = half ** (-0.5)
    inputs[2].wait()
    split(2, store_rows)
    for h in range(heads):
        columns = turned(h) * scale
        qs[h, :, 0:toks] = jnp.where(depth < half, columns, 0.0).astype(BF16)
        qs[h, :, toks:] = jnp.where(depth >= half, columns, 0.0).astype(BF16)
    highs[...] = jnp.full_like(highs, -1e30)
    totals[...] = jnp.zeros_like(totals)
    acc[...] = jnp.zeros_like(acc)
    rows = lax.broadcasted_iota(jnp.int32, (toks, toks), 0)
    cols = lax.broadcasted_iota(jnp.int32, (toks, toks), 1)
    eye = rows == cols

    def process(b, masked):
        for h in range(heads):
            scores = mixed_dot(kall[b, head_rows(h), :], qs[h], ((1,), (0,)))
            if masked:
                scores = jnp.where(jnp.concatenate([rows <= cols] * 2, axis=1), scores, -1e30)
            old = highs[h]
            high = jnp.maximum(old, jnp.max(scores, axis=0, keepdims=True))
            shrink = jnp.exp(old - high)
            weights = jnp.exp(scores - high)
            totals[h] = shrink * totals[h] + jnp.sum(weights, axis=0, keepdims=True)
            blended = mixed_dot(
                vall[b, h * head_width : (h + 1) * head_width, :], weights.astype(BF16),
                ((1,), (0,)),
            )
            acc[h] = shrink * acc[h] + blended
            highs[h] = high

    with SC('proc_own'):
        process(sp, True)

    for load in small:
        load.wait()
    first = route_ref[0:1, :]
    lead = lax.broadcasted_iota(jnp.int32, (8, toks), 0)
    member = jnp.logical_and(
        first >= lead * per_group, first < (lead + 1) * per_group
    ).astype(F32)
    earlier = mixed_dot(member.astype(BF16), (rows < cols).astype(BF16), ((1,), (0,)))
    slot = jnp.sum(member * (earlier + lead.astype(F32) * cap), axis=0, keepdims=True)
    slot_col = jnp.sum(jnp.where(eye, slot, 0.0), axis=1, keepdims=True)
    slots = GROUPS * cap
    sel[...] = (
        lax.broadcasted_iota(jnp.int32, (slots, toks), 0) == slot.astype(jnp.int32)
    ).astype(BF16)
    selt[...] = (
        lax.broadcasted_iota(jnp.int32, (toks, slots), 1) == slot_col.astype(jnp.int32)
    ).astype(BF16)
    names = lax.broadcasted_iota(jnp.int32, (experts, toks), 0)
    by_expert = jnp.zeros((experts, toks), F32)
    for k in range(route_ref.shape[0]):
        by_expert = by_expert + jnp.where(
            names == route_ref[k : k + 1, :], rw_ref[k : k + 1, :], 0.0
        )
    by_slot = exact_pick(by_expert, selt[...])
    table = by_slot[:, 0:cap]
    for g in range(1, GROUPS):
        table = table + by_slot[:, g * cap : (g + 1) * cap]
    meta[sp, 0:experts, :] = table

    @pl.when(c == 1)
    def _():
        kv_sib_copy(2 * z).wait_recv()
        process(2 * z, False)

    def give_credits(j):
        def credit(which, plane):
            pl.semaphore_signal(
                free_sem.at[which], inc=1, device_id={"sp": 2 * plane + c, "tp": tp},
                device_id_type=MESH,
            )

        @pl.when(jnp.logical_and(j == z, z == zs - 2))
        def _():
            credit(0, 0)

        @pl.when(jnp.logical_and(j == z, z == zs - 1))
        def _():
            credit(1, 0)
            credit(1, 1)

    def visit(j, carry):
        b = 2 * (z - j) + c
        other = 2 * (z - j) + 1 - c
        with SC('wait_b'):
            kv_sib_copy(b).wait_recv()

        @pl.when(z < zs - 1)
        def _():
            next_copy(b).start()

        kv_sib_copy(b).start()
        give_credits(j)
        with SC('proc_b'):
            process(b, False)
        with SC('wait_o'):
            kv_sib_copy(other).wait_recv()
        with SC('proc_o'):
            process(other, False)
        return carry

    lax.fori_loop(1, z + 1, visit, 0)

    for h in range(heads):
        blend = acc[h] * (1.0 / totals[h])
        mix = blend[:, :toks] - lam_ref[:, h : h + 1] * blend[:, toks:]
        mix = mix * lax.rsqrt(jnp.mean(mix * mix, axis=0, keepdims=True) + norm_eps)
        att[:, h * head_width : (h + 1) * head_width] = (mix.T * gain_ref[...]).astype(BF16)
    inputs[3].wait()

    def projected(to):
        return jnp.dot(
            att[...], owv[:, pl.ds(pl.multiple_of(to * piece, piece), piece)],
            preferred_element_type=F32,
        )

    half_toks = toks // 2
    part_halves = (slice(0, half_toks), slice(half_toks, toks))

    def rs_copy(i):
        to, source, target = [
            (beside, part.at[across, part_halves[0]], ppass.at[0]),
            (above, part.at[across, part_halves[1]], ppass.at[1]),
            (beside, part.at[beside, part_halves[0]], rbuf.at[0, part_halves[0]]),
            (above, part.at[above, part_halves[1]], rbuf.at[1, part_halves[1]]),
            (above, part.at[above, part_halves[0]], rbuf.at[1, part_halves[0]]),
            (beside, part.at[beside, part_halves[1]], rbuf.at[0, part_halves[1]]),
        ][i]
        return remote(source, target, rs_send, rs_recv.at[min(i, 2)], sp, to)

    part[across] = projected(across).astype(BF16)
    rs_copy(0).start()
    rs_copy(1).start()
    for_beside = projected(beside)
    part[beside, part_halves[0]] = for_beside[part_halves[0]].astype(BF16)
    rs_copy(2).start()
    for_above = projected(above)
    part[above, part_halves[1]] = for_above[part_halves[1]].astype(BF16)
    rs_copy(3).start()
    mine = pl.ds(pl.multiple_of(tp * piece, piece), piece)
    inputs[4].wait()
    total = resv[:, mine].astype(F32) + projected(tp)
    with SC("rs_pass"):
        rs_copy(0).wait_recv()
    part[above, part_halves[0]] = (for_above[part_halves[0]] + ppass[0].astype(F32)).astype(BF16)
    rs_copy(4).start()
    with SC("rs_pass"):
        rs_copy(1).wait_recv()
    part[beside, part_halves[1]] = (for_beside[part_halves[1]] + ppass[1].astype(F32)).astype(BF16)
    rs_copy(5).start()
    wd_start(2)

    half_cap = cap // 2

    def spot(src, core, part):
        return xall.at[
            src,
            pl.ds(pl.multiple_of(core * cap, cap), cap),
            pl.ds(pl.multiple_of(part * piece, piece), piece),
        ]

    def half_spot(src, part, side):
        return xall.at[
            src,
            pl.ds(pl.multiple_of(c * cap + side * half_cap, half_cap), half_cap),
            pl.ds(pl.multiple_of(part * piece, piece), piece),
        ]

    def x_copy(s):
        group = (z + s) % zs
        return remote(
            xs.at[s], spot(z, c, tp), x_send, x_recv.at[z, 0], 2 * group + c, tp
        )

    def spot_wait(here, sem):
        remote(here, here, x_send, sem, sib, tp).wait_recv()

    def tp_copy(src, i):
        to, side = [(beside, 0), (above, 1), (beside, 1), (above, 0)][i]
        here = half_spot(src, tp, side)
        return remote(here, here, x_tp, x_recv.at[src, 1 + i // 2], sp, to)

    def pass_copy(src, i):
        part, side, to = [(beside, 0, above), (above, 1, beside)][i]
        here = half_spot(src, part, side)
        return remote(here, here, x_tp, x_recv.at[src, 3], sp, to)

    def sib_copy(src, part):
        here = spot(src, c, part)
        return remote(here, here, x_sib, s_recv.at[src], sib, tp)

    def gather(src):
        @pl.when(src != z)
        def _():
            with SC("arrive"):
                spot_wait(spot(src, c, tp), x_recv.at[src, 0])

        for i in range(4):
            tp_copy(src, i).start()
        sib_copy(src, tp).start()

    def gather_pass(src):
        with SC("gpass"):
            spot_wait(spot(src, c, beside), x_recv.at[src, 1])
        pass_copy(src, 0).start()
        pass_copy(src, 1).start()

    def forward(src):
        with SC("compl_tp"):
            spot_wait(spot(src, c, beside), x_recv.at[src, 2])
            sib_copy(src, beside).start()
            sib_copy(src, above).start()
            spot_wait(spot(src, c, across), x_recv.at[src, 3])
            sib_copy(src, across).start()

    def complete(src):
        with SC("compl_sib"):
            spot_wait(
                xall.at[src, pl.ds(pl.multiple_of((1 - c) * cap, cap), cap)], s_recv.at[src]
            )

    pl.when(z > 0)(lambda: gather(0))
    pl.when(z == zs - 2)(lambda: gather(1))

    with SC("rs_wait"):
        remote(rbuf, rbuf, rs_send, rs_recv.at[2], sp, beside).wait_recv()
    total = total + rbuf[0].astype(F32) + rbuf[1].astype(F32)
    stream_ref[...] = total
    normed_ref[...] = (total * fg_ref[:, mine]).astype(BF16)
    squares = jnp.sum(total * total, axis=1, keepdims=True)
    as_row = jnp.sum(jnp.where(eye, squares, 0.0), axis=0, keepdims=True)
    sq_send[...] = jnp.broadcast_to(as_row, sq_send.shape)

    def sq_copy(d):
        return remote(
            sq_send, sq_recv.at[d], sq_ss, sq_rs, sp, (tp + d) % tps
        )

    for d in range(1, tps):
        sq_copy(d).start()

    def m_copy(d):
        return remote(meta.at[sp], meta.at[sp], m_send, m_recv.at[sp], (sp + d) % n, tp)

    def m_wait(src):
        @pl.when(src != sp)
        def _():
            remote(meta.at[src], meta.at[src], m_send, m_recv.at[src], sib, tp).wait_recv()

    for s in list(range(1, zs)) + [0]:
        group = (z + s) % zs
        picked = jnp.dot(
            sel[pl.ds(pl.multiple_of(group * cap, cap), cap), :], normed_ref[...],
            preferred_element_type=F32,
        ).astype(BF16)
        if s:
            xs[s] = picked
            pl.when(z >= (zs - s if s >= zs - 2 else 0))(lambda: x_copy(s).start())
        else:
            spot(z, c, tp)[...] = picked

    @pl.when(z < zs - 1)
    def _():
        gather(z)

    wd_start(3)

    def row_factors():
        with SC("sq_wait"):
            squares_in = sq_recv.at[pl.ds(1, tps - 1)]
            remote(squares_in, squares_in, sq_ss, sq_rs, sp, beside).wait_recv()
        sums = sq_send[0:1, :]
        for d in range(1, tps):
            sums = sums + sq_recv[d, 0:1, :]
        inverse = lax.rsqrt(sums * (1.0 / (piece * tps)) + norm_eps)
        by_slot = exact_pick(jnp.broadcast_to(inverse, (8, toks)), selt[...])
        for g in range(GROUPS):
            meta[sp, experts + g : experts + g + 1, :] = by_slot[0:1, g * cap : (g + 1) * cap]
        for d in range(1, n):
            m_copy(d).start()

    def late_rows(s, which):
        with SC("credit"):
            pl.semaphore_wait(free_sem.at[which], 1)
        x_copy(s).start()

    pl.when(z < zs - 2)(row_factors)
    gather_pass(0)

    @pl.when(z == zs - 2)
    def _():
        gather_pass(1)
        gather_pass(2)

    pl.when(z == zs - 1)(lambda: gather(1))
    wd_start(4)
    pl.when(z == zs - 2)(row_factors)
    pl.when(z == 1)(lambda: late_rows(zs - 2, 1))

    @pl.when(z == 0)
    def _():
        late_rows(zs - 2, 0)
        gather(1)
        late_rows(zs - 1, 1)

    def late_sources():
        gather(zs - 2)
        pl.when(z == 0)(lambda: gather_pass(1))
        wd_start(5)
        forward(1)
        gather_pass(zs - 2)
        wd_start(6)

    def near_copy(src, part):
        return remote(
            away.at[src, part], near.at[src, part], n_send,
            n_recv.at[src, jnp.where(part == across, 0, 1)], sib, tp,
        )

    def near_wait(src, first):
        here = near.at[src, pl.ds(0, 1 if first else tps - 1)]
        remote(here, here, n_send, n_recv.at[src, 0 if first else 1], sib, tp).wait_recv()

    tile = 512
    small_eye = lax.broadcasted_iota(jnp.int32, (cap, cap), 0) == lax.broadcasted_iota(
        jnp.int32, (cap, cap), 1
    )
    which = lax.broadcasted_iota(jnp.int32, meta.shape[1:], 0)

    def meta_col(src, core, line):
        row = jnp.sum(jnp.where(which == line, meta[2 * src + core], 0.0), axis=0, keepdims=True)
        return jnp.sum(jnp.where(small_eye, row, 0.0), axis=1, keepdims=True)

    keep_rows = pl.ds(pl.multiple_of(c * cap, cap), cap)
    away_rows = pl.ds(pl.multiple_of((1 - c) * cap, cap), cap)

    def ffn_one(src, between):
        @pl.when(src == 0)
        def _():
            for load in loads:
                load.wait()

        with SC("m_wait"):
            m_wait(2 * src)
            m_wait(2 * src + 1)
        factor = jnp.concatenate(
            [meta_col(src, c, experts + z), meta_col(src, 1 - c, experts + z)], axis=0
        )

        def one(i, carry):
            pl.when(i == wg.shape[1] // tile // 2)(between)
            at = pl.ds(pl.multiple_of(i * tile, tile), tile)
            x = jnp.concatenate([xall[src, keep_rows], xall[src, away_rows]], axis=0)
            gate = jnp.dot(x, wg[:, at], preferred_element_type=F32) * factor
            up = jnp.dot(x, wu[:, at], preferred_element_type=F32) * factor
            hid[src, :, at] = (gate / (1.0 + jnp.exp(-gate)) * up).astype(BF16)
            return carry

        with SC("ffn_one"):
            lax.fori_loop(0, wg.shape[1] // tile, one, 0)

    def ffn_two(src, first):
        @pl.when(first)
        def _():
            with SC("down_wait"):
                others = wdv.at[pl.ds(0, tps - 1)]
                remote(others, others, wd_send, wd_recv, sp, beside).wait()

        row_weight = jnp.concatenate(
            [meta_col(src, c, sp), meta_col(src, 1 - c, sp)], axis=0
        )

        def two(j, carry):
            to = tp ^ (tps - 1 - j)
            result = jnp.dot(hid[src], wdv[to], preferred_element_type=F32) * row_weight
            away[src, to] = result[cap:].astype(BF16)
            near_copy(src, to).start()
            keep[src, to] = result[:cap]
            return carry

        with SC("ffn_two"):
            for j in range(tps):
                two(j, 0)

    cap_halves = (slice(0, half_cap), slice(half_cap, cap))

    def r_copy(src, i):
        to, source, target = [
            (beside, rsend.at[src, across, cap_halves[0]], rpass.at[src, 0]),
            (above, rsend.at[src, across, cap_halves[1]], rpass.at[src, 1]),
            (beside, rsend.at[src, beside, cap_halves[0]], rrecv.at[src, 0, cap_halves[0]]),
            (above, rsend.at[src, above, cap_halves[1]], rrecv.at[src, 1, cap_halves[1]]),
            (above, rsend.at[src, above, cap_halves[0]], rrecv.at[src, 1, cap_halves[0]]),
            (beside, rsend.at[src, beside, cap_halves[1]], rrecv.at[src, 0, cap_halves[1]]),
        ][i]
        return remote(source, target, r_send, r_recv.at[src, min(i // 2, 1)], sp, to)

    def both(src, to, at):
        return keep[src, to, at, :] + near[src, to, at, :].astype(F32)

    def spread(src):
        with SC("near_wait"):
            near_wait(src, True)
        rsend[src, across] = both(src, across, slice(0, cap)).astype(BF16)
        r_copy(src, 0).start()
        r_copy(src, 1).start()
        near_wait(src, False)
        rsend[src, above, cap_halves[1]] = both(src, above, cap_halves[1]).astype(BF16)
        r_copy(src, 3).start()
        rsend[src, beside, cap_halves[0]] = both(src, beside, cap_halves[0]).astype(BF16)
        r_copy(src, 2).start()

    def spread_pass(src):
        with SC("spass"):
            passed = rpass.at[src]
            remote(passed, passed, r_send, r_recv.at[src, 0], sp, beside).wait_recv()
        rsend[src, above, cap_halves[0]] = (
            both(src, above, cap_halves[0]) + rpass[src, 0].astype(F32)
        ).astype(BF16)
        r_copy(src, 4).start()
        rsend[src, beside, cap_halves[1]] = (
            both(src, beside, cap_halves[1]) + rpass[src, 1].astype(F32)
        ).astype(BF16)
        r_copy(src, 5).start()

    def b_copy(src):
        return remote(
            back.at[src], ret.at[z], b_send, b_recv, 2 * src + c, tp
        )

    def finish(src):
        with SC("r_wait"):
            here = rrecv.at[src]
            remote(here, here, r_send, r_recv.at[src, 1], sp, beside).wait_recv()
        total = both(src, tp, slice(0, cap))
        total = total + rrecv[src, 0].astype(F32) + rrecv[src, 1].astype(F32)

        @pl.when(src == z)
        def _():
            ret[z] = total.astype(BF16)

        @pl.when(src != z)
        def _():
            back[src] = total.astype(BF16)
            b_copy(src).start()

    last = zs - 1

    at_last = z == last

    early = z < last

    def when_both(one, two):
        return pl.when(jnp.logical_and(one, two))

    third = z == last - 1
    first_two = z < last - 1
    lead = jnp.where(first_two, last - 1, 0)
    after = jnp.where(z == 1, 0, 1)

    def up_step(s):
        def between():
            when_both(third, s == 0)(lambda: forward(1))
            when_both(z == 1, s == 0)(lambda: gather_pass(1))
            when_both(early, s == 1)(lambda: forward(2))
            when_both(early, s == last - 1)(lambda: gather(last))
            when_both(early, s == last)(lambda: finish(lead))
            when_both(early, s == last)(lambda: spread_pass(after))
            when_both(at_last, s < last)(lambda: gather_pass(s + 1))
            when_both(at_last, s + 2 <= last)(lambda: gather(s + 2))

        pl.when(s == 0)(lambda: forward(0))
        when_both(at_last, s == 0)(row_factors)
        when_both(first_two, s == 1)(late_sources)
        complete(s)
        ffn_one(s, between)
        when_both(at_last, s == last)(lambda: spread_pass(last - 1))

    def down_step(s):
        ffn_two(s, s == jnp.where(early, lead, 0))
        when_both(at_last, s < last)(lambda: forward(s + 1))
        when_both(early, s == lead)(lambda: gather_pass(last))
        when_both(early, s == after)(lambda: spread_pass(lead))
        when_both(early, s == z)(lambda: spread_pass(last))
        when_both(at_last, jnp.logical_and(s >= 1, s < last))(lambda: spread_pass(s - 1))
        spread(s)
        when_both(early, s == after)(lambda: forward(last))
        when_both(early, s == last)(lambda: finish(after))
        when_both(at_last, s == last - 1)(lambda: finish(0))

        @pl.when(jnp.logical_and(at_last, s == last))
        def _():
            finish(1)
            finish(2)

    def step(k, carry):
        turn = k
        for at, value in enumerate(
            (0, 2, 4, 2 * lead + 1, 2 * after + 1, 2 * last, 2 * last + 1, 2 * z + 1)
        ):
            turn = jnp.where(jnp.logical_and(early, k == at), value, turn)
        pl.when(turn % 2 == 0)(lambda: up_step(turn // 2))
        pl.when(turn % 2 == 1)(lambda: down_step(turn // 2))
        return carry

    lax.fori_loop(0, 2 * zs, step, 0)
    pl.when(at_last)(lambda: spread_pass(last))
    finish(last)

    @pl.when(early)
    def _():
        spread_pass(z)
        finish(z)

    with SC("b_wait"):
        returns = ret.at[pl.ds(0, zs - 1)]
        remote(returns, returns, b_send, b_recv, sib, tp).wait_recv()
    rows = ret[...].reshape(zs * cap, piece)
    layer = stream_ref[...] + jnp.dot(selt[...], rows, preferred_element_type=F32)
    outv[:, mine] = layer.astype(BF16)

    def out_spot(part, side):
        return outv.at[part_halves[side], pl.ds(pl.multiple_of(part * piece, piece), piece)]

    def o_copy(i):
        part, side, to = [
            (tp, 0, beside), (tp, 1, above), (tp, 1, beside), (tp, 0, above),
            (beside, 0, above), (above, 1, beside),
        ][i]
        here = out_spot(part, side)
        return remote(here, here, o_send, o_recv.at[min(i, 4)], sp, to)

    def o_wait(part, i, side=None):
        at = pl.ds(pl.multiple_of(part * piece, piece), piece)
        here = outv.at[:, at] if side is None else out_spot(part, side)
        remote(here, here, o_send, o_recv.at[i], sib, tp).wait_recv()

    for i in range(4):
        o_copy(i).start()
    with SC("o_pass"):
        o_wait(beside, 0, 0)
    o_copy(4).start()
    with SC("o_pass"):
        o_wait(above, 1, 1)
    o_copy(5).start()

    def sent(here, sem):
        remote(here, here, sem, kv_recv.at[0], sib, tp).wait_send()

    sent(sq_recv.at[pl.ds(1, tps - 1)], sq_ss)
    sent(part.at[pl.ds(0, 3)], rs_send)
    sent(meta.at[pl.ds(0, n - 1)], m_send)
    sent(xs.at[pl.ds(1, zs - 1)], x_send)
    sent(back.at[pl.ds(0, zs - 1)], b_send)
    sent(away, n_send)
    sent(away, x_sib)
    sent(away.at[pl.ds(0, zs - 1)], x_tp)
    sent(away.at[pl.ds(0, zs - 1)], r_send)

    @pl.when(z < zs - 1)
    def _():
        next_copy(sp).wait_send()

    @pl.when(c == 0)
    def _():
        kv_sib_copy(sp).wait_send()

    def drain(j, carry):
        b = 2 * (z - j) + c

        @pl.when(z < zs - 1)
        def _():
            next_copy(b).wait_send()

        kv_sib_copy(b).wait_send()
        return carry

    lax.fori_loop(1, z + 1, drain, 0)
    with SC("o_wait"):
        o_wait(beside, 2, 1)
        o_wait(above, 3, 0)
        o_wait(across, 4)
    with SC("o_send"):
        sent(part.at[pl.ds(0, 3)], o_send)


def paired_shards(
    residual, queries, key_vectors, value_rows, head_lambda, head_gain, out_weight, ffn_gain,
    expert_gate, expert_up, expert_down, routing, route_weight,
):
    n = lax.axis_size("sp")
    tps = lax.axis_size("tp")
    toks, heads, head_width = queries.shape
    width = heads * head_width
    model = residual.shape[1]
    piece = model // tps
    experts = n
    per_group = experts // GROUPS
    cap = toks // per_group
    down = expert_down[0]
    wd_rows = down.shape[0] // tps
    vmem = pl.BlockSpec(memory_space=pltpu.VMEM)
    hbm = pl.BlockSpec(memory_space=pltpu.HBM)
    dma = pltpu.SemaphoreType.DMA
    zs = n // 2
    def stay(x):
        return pltpu.with_memory_space_constraint(x, pltpu.HBM)

    return pl.pallas_call(
        functools.partial(layer_kernel, n, tps, cap, heads, head_width),
        out_shape=jax.ShapeDtypeStruct((toks, model), BF16),
        in_specs=[hbm] * 13,
        out_specs=vmem,
        scratch_shapes=[
            pltpu.VMEM(routing.shape[::-1], jnp.int32),
            pltpu.VMEM(route_weight.shape[::-1], F32),
            pltpu.VMEM((1, heads), F32),
            pltpu.VMEM((1, head_width), F32),
            pltpu.VMEM((1, model), F32),
            pltpu.VMEM((3, toks * heads, head_width), BF16),
            pltpu.VMEM((toks, model), BF16),
            pltpu.VMEM((width, model), BF16),
            pltpu.VMEM((GROUPS * cap, toks), BF16),
            pltpu.VMEM((toks, GROUPS * cap), BF16),
            pltpu.VMEM((toks, piece), F32),
            pltpu.VMEM((toks, piece), BF16),
            pltpu.VMEM((n, experts + 8, cap), F32),
            pltpu.VMEM((zs, cap, piece), BF16),
            pltpu.VMEM((zs, 2 * cap, model), BF16),
            pltpu.VMEM(expert_gate.shape[1:], BF16),
            pltpu.VMEM(expert_up.shape[1:], BF16),
            pltpu.VMEM((tps, wd_rows, piece), BF16),
            pltpu.VMEM((zs, 2 * cap, expert_gate.shape[2]), BF16),
            pltpu.VMEM((zs, tps, cap, piece), F32),
            pltpu.VMEM((zs, tps, cap, piece), BF16),
            pltpu.VMEM((zs, tps, cap, piece), BF16),
            pltpu.VMEM((zs, tps, cap, piece), BF16),
            pltpu.VMEM((zs, 2, cap, piece), BF16),
            pltpu.VMEM((zs, 2, cap // 2, piece), BF16),
            pltpu.VMEM((zs, cap, piece), BF16),
            pltpu.VMEM((zs, cap, piece), BF16),
            pltpu.VMEM((n, heads * toks, head_width), BF16),
            pltpu.VMEM((n, width, toks), BF16),
            pltpu.VMEM((heads * toks, head_width), BF16),
            pltpu.VMEM((heads, head_width, 2 * toks), BF16),
            pltpu.VMEM((heads, 1, 2 * toks), F32),
            pltpu.VMEM((heads, 1, 2 * toks), F32),
            pltpu.VMEM((heads, head_width, 2 * toks), F32),
            pltpu.VMEM((toks, width), BF16),
            pltpu.VMEM((tps, toks, piece), BF16),
            pltpu.VMEM((2, toks, piece), BF16),
            pltpu.VMEM((2, toks // 2, piece), BF16),
            pltpu.VMEM((8, toks), F32),
            pltpu.VMEM((tps, 8, toks), F32),
            dma((10,)), dma((3,)),
            dma, dma, dma, dma((zs, 4)), dma((zs,)),
            dma, dma((zs, 2)), dma, dma((zs, 2)),
            dma, dma, dma, dma((5,)),
            dma((zs,)), dma((zs,)), dma((n,)),
            dma, dma, dma, dma((n,)),
            dma, dma((3,)), dma, dma, pltpu.SemaphoreType.REGULAR((2,)),
        ],
        compiler_params=pltpu.CompilerParams(collective_id=0, has_side_effects=True, vmem_limit_bytes=49545216),
        name="layer",
    )(
        stay(queries.reshape(toks * heads, head_width)), stay(key_vectors.reshape(toks * heads, head_width)),
        stay(value_rows.reshape(toks * heads, head_width)), stay(routing.T), stay(route_weight.T), stay(down),
        stay(head_lambda.reshape(1, -1)), stay(head_gain.reshape(1, -1)), stay(out_weight), stay(residual), stay(ffn_gain.reshape(1, -1)),
        stay(expert_gate), stay(expert_up),
    )


def solution(mesh):
    in_specs = (
        P("sp", None),
        P("sp", "tp", None),
        P("sp", "tp", None),
        P("sp", "tp", None),
        P("tp"),
        P(),
        P("tp", None),
        P(),
        P("sp", None, "tp"),
        P("sp", None, "tp"),
        P("sp", None, "tp"),
        P("sp", None),
        P("sp", None),
    )
    out_specs = P("sp", None)
    paired = mesh.shape["sp"] == 2 * GROUPS and mesh.shape["tp"] == 4
    return jax.shard_map(paired_shards if paired else shards, mesh=mesh, in_specs=in_specs, out_specs=out_specs, check_vma=False)
```
